128 devices in a mesh: ep: 64 (over z, y, x), tp: 2 (over core).
Axes of the slice: x: 4, y: 4, z: 4, core: 2. Of those that a mesh axis runs over, the one named last changes fastest.
Arguments:
- tokens: bfloat16 [32768, 2048], P(('ep', 'tp')), may hold values from -6 to 6
- norm_gain: float32 [2048], replicated, may hold values from 0.1 to 1.9
- norm_bias: float32 [2048], replicated, may hold values from -3 to 3
- gate_weight: bfloat16 [64, 2048, 1024], P('ep', None, 'tp'), may hold values from -0.125 to 0.125
- up_weight: bfloat16 [64, 2048, 1024], P('ep', None, 'tp'), may hold values from -0.125 to 0.125
- down_weight: bfloat16 [64, 1024, 2048], P('ep', 'tp'), may hold values from -0.1875 to 0.1875
- expert_ids: int32 [32768, 2], P(('ep', 'tp')), may hold values from 0 to 63, all different within a row; in each aligned block of 256 rows (0 to 255, 256 to 511, ...) at most 16 rows name the same one
- route_weights: float32 [32768, 2], P(('ep', 'tp')), may hold values from 0.2 to 1
Outputs:
- mixed: bfloat16 [32768, 2048], P(('ep', 'tp'))
The draws below stay inside these ranges and needn't reach their ends.
Inputs may be any that keep to these rules, and one draw needn't show every extreme that they name: `expert_ids`: a token's 2 experts differ; in the tokens of one device (aligned blocks of 256 rows) no expert is named by more than 16 entries, a bound that some block reaches.
All inputs are finite; a program needn't handle non-finite values.
Results may differ from the reference program's by a relative error of at most 0.0071.
Values may be sent and summed in bfloat16 or wider, within the bound.
A program may use at most 128 MiB of HBM per device.

```python
import math
import jax
import jax.numpy as jnp
import numpy as np
from jax import lax

D = 2048
FFE = 1024
TOPK = 2
TOK_DEV = 256
EXPERTS = 64
CAP = 16
TOKENS = 32768


def block_scale(key, dims, cuts, least, high):
    def one(dim, shards_of):
        draws = jax.random.uniform(jax.random.fold_in(jax.random.fold_in(key, 6), dim), (shards_of,), jnp.float32, least / len(cuts), high / len(cuts))
        return jnp.repeat(jnp.exp(draws), dims[dim] // shards_of).reshape((-1,) + (1,) * (len(dims) - dim - 1))

    level = one(*cuts[0])
    for cut in cuts[1:]:
        level = level * one(*cut)
    return level


def assign_block(stream_key, own, number, rows, number_of, top, limit, skew):
    ranking = jax.random.permutation(stream_key, number_of)
    heavy_load, common = shares(number_of, rows * top, limit, skew, True), shares(number_of, rows * top, limit, skew, False)
    places = jnp.arange(number_of)

    def named(tallies, offset_by):
        used = int((tallies > 0).sum())
        fixed = max(1, used // 4)
        moved = fixed + (places - fixed + offset_by * (used - fixed)) % max(1, number_of - fixed)
        return jnp.zeros((number_of,), jnp.int32).at[ranking[jnp.where(places < fixed, places, moved)]].set(jnp.asarray(tallies, jnp.int32))

    tallies = jnp.where(number % 4 == 0, named(heavy_load, number // 4), named(common, number - number // 4 - 1))
    mixed = jax.random.permutation(jax.random.fold_in(own, 3), number_of)
    source_of, receiver = mixed[0:number_of // 2 * 2:2], mixed[1:number_of // 2 * 2:2]
    room = jnp.minimum(tallies[source_of] - 1, limit - tallies[receiver]) // 2
    room = jnp.where((source_of == ranking[0]) | (receiver == ranking[0]) | (tallies[receiver] == 0), 0, jnp.maximum(room, 0))
    moved = jax.random.randint(jax.random.fold_in(own, 4), (number_of // 2,), 0, 1 << 20) % (room + 1)
    tallies = tallies.at[source_of].add(-moved).at[receiver].add(moved)
    members = jnp.searchsorted(jnp.cumsum(tallies), jnp.arange(rows * top), side="right").astype(jnp.int32)
    grid = members.reshape(top, rows).T
    grid = grid[jax.random.permutation(jax.random.fold_in(own, 1), rows)]
    offset_by = jax.random.randint(jax.random.fold_in(own, 2), (rows, 1), 0, top)
    return jnp.take_along_axis(grid, (jnp.arange(top)[None, :] + offset_by) % top, axis=1)


def shares(number_of, total, bound, slope, full):
    loads = [(1 << 20) // math.isqrt(rank ** slope) + 1 for rank in range(1, number_of + 1)]
    largest = bound if full else min(bound, max(-(-total // number_of), total * loads[0] // sum(loads)))
    least = 1 if total - largest >= number_of - 1 else 0
    counts, rest = [largest] + [least] * (number_of - 1), total - largest - least * (number_of - 1)
    while rest > 0:
        candidates = [i for i in range(1, number_of) if counts[i] < largest] or [i for i in range(1, number_of) if counts[i] < bound]
        pool, left = sum([loads[i] for i in candidates]), rest
        for i in candidates:
            more = min(bound - counts[i], max(1, left * loads[i] // pool), rest)
            counts[i] = counts[i] + more
            rest = rest - more
    return np.array(counts)


def scatter_about(own_key, shape, width, bound, cuts=(), held_as=jnp.bfloat16):
    array = jax.random.normal(own_key, shape, jnp.float32) * width
    if len(cuts) > 0:
        array = block_scale(own_key, shape, cuts, -0.22, 0.18) * array
    return jnp.clip(array, min=-bound, max=bound).astype(held_as)


def setup_inputs(seed: int = 0) -> dict:
    seeds = jax.random.split(jax.random.key(seed), 9)
    tokens = scatter_about(seeds[0], (TOKENS, D), 1.0, 6.0, ((0, 128),))
    norm_gain = jnp.clip(1.0 + 0.18 * jax.random.normal(seeds[1], (D,), jnp.float32), 0.1, 1.9)
    norm_bias = scatter_about(seeds[2], (D,), 0.5, 3.0, (), jnp.float32)
    gate_weight = scatter_about(seeds[3], (EXPERTS, D, FFE), D ** -0.5, 0.125, ((0, 64), (2, 2)))
    up_weight = scatter_about(seeds[4], (EXPERTS, D, FFE), D ** -0.5, 0.125, ((0, 64), (2, 2)))
    down_weight = scatter_about(seeds[5], (EXPERTS, FFE, D), FFE ** -0.5, 0.1875, ((0, 64), (1, 2)))
    expert_ids_keys = jax.random.split(jax.random.fold_in(seeds[6], 1), TOKENS // TOK_DEV)
    expert_ids_turns = jax.random.permutation(jax.random.fold_in(seeds[6], 3), TOKENS // TOK_DEV)
    expert_ids = jax.vmap(lambda own, number: assign_block(jax.random.fold_in(seeds[6], 2), own, number, TOK_DEV, EXPERTS, TOPK, CAP, 2))(expert_ids_keys, expert_ids_turns).reshape((TOKENS, TOPK))
    route_weights = jnp.clip(0.2 + 0.8 * jax.random.uniform(seeds[7], (TOKENS, TOPK), jnp.float32) ** block_scale(seeds[7], (TOKENS, TOPK), ((0, 128),), -0.2, 0.2), 0.2, 1.0)
    return {"tokens": tokens, "norm_gain": norm_gain, "norm_bias": norm_bias, "gate_weight": gate_weight, "up_weight": up_weight, "down_weight": down_weight, "expert_ids": expert_ids, "route_weights": route_weights}


def expert_rows(rows, w_gate, w_up, w_down):
    gate = jnp.dot(rows, w_gate, preferred_element_type=jnp.float32)
    upper = jnp.dot(rows, w_up, preferred_element_type=jnp.float32)
    hidden = (jax.nn.silu(gate) * upper).astype(jnp.bfloat16)
    return jnp.dot(hidden, w_down, preferred_element_type=jnp.float32).astype(jnp.bfloat16)

def reference(tokens, norm_gain, norm_bias, gate_weight, up_weight, down_weight, expert_ids, route_weights):
    values = tokens.astype(jnp.float32)
    centre = values - lax.optimization_barrier(jnp.mean(values, axis=-1, keepdims=True))
    spread = lax.optimization_barrier(jnp.mean(centre * centre, axis=-1, keepdims=True))
    normed = (centre * lax.rsqrt(spread + 1e-05) * norm_gain + norm_bias).astype(jnp.bfloat16)
    sources = TOKENS // TOK_DEV
    blocks = expert_ids.reshape(sources, TOK_DEV * TOPK)
    onehot = (blocks[:, :, None] == jnp.arange(EXPERTS, dtype=jnp.int32)[None, None, :]).astype(jnp.int32)
    slot = lax.optimization_barrier(jnp.sum(jnp.cumsum(onehot, axis=1) * onehot, axis=-1)) - 1
    row_index = (jnp.arange(sources, dtype=jnp.int32)[:, None] * CAP + slot).reshape(-1).astype(jnp.int32)
    flat_ids = expert_ids.reshape(-1)
    token_rows = jnp.repeat(normed, TOPK, axis=0)
    buffer_rows = sources * CAP

    def one_expert(expert, total):
        chosen = flat_ids == expert
        index = jnp.where(chosen, row_index, buffer_rows).astype(jnp.int32)
        buffer = jnp.zeros((buffer_rows, D), jnp.bfloat16).at[index].set(token_rows, mode='drop')
        result = expert_rows(buffer, gate_weight[expert], up_weight[expert], down_weight[expert])
        picked = result[jnp.minimum(index, buffer_rows - 1)]
        picked = jnp.where(chosen[:, None], picked.astype(jnp.float32), 0.0).reshape(TOKENS, TOPK, D)
        return total + lax.optimization_barrier(jnp.sum(picked * route_weights[:, :, None], axis=1))
    total = lax.fori_loop(0, EXPERTS, one_expert, jnp.zeros((TOKENS, D), jnp.float32))
    return total.astype(jnp.bfloat16)
```

```python
import functools

import jax
import jax.numpy as jnp
from jax import lax
from jax.experimental import pallas as pl
from jax.experimental.pallas import tpu as pltpu
from jax.sharding import PartitionSpec as P

MESH = pl.DeviceIdType.MESH
LINE = 4
CHUNKS = 8
HALF = CHUNKS // 2


def kernel(
    planes, raw, gain, bias, idsin, wtin, gw, uw, dw, out,
    src, gn, bs, ids, wts, tok, met, wg, wu, wd, sel, mix, snd, xin, hid, res, ret, psend, racc,
    fin, s_own, s_met, s_mets, s_wl, s_ws, s_wr, s_tok, s_toks, s_x, s_xs, s_r, s_rs, s_p, s_ps, s_o,
):
    n = LINE
    side = planes
    me, core = lax.axis_index("ep"), lax.axis_index("tp")
    z, p = me // side, lax.rem(me, side)
    tokens, width = raw.shape
    half = gw.shape[2]
    rows = snd.shape[1]
    cap = rows // side
    k = CHUNKS
    wide = width // k

    def cols(c):
        return pl.ds(pl.multiple_of(c * wide, wide), wide)

    def band(i):
        return pl.ds(pl.multiple_of(i * cap, cap), cap)

    def plane(j):
        return {"ep": lax.rem(z + j, n) * side + p}

    up, over, back = 1, 2, n - 1

    def peer(j):
        return lax.rem(p + j, side)

    def remote(src, dst, send, recv, where):
        return pltpu.make_async_remote_copy(
            src_ref=src, dst_ref=dst, send_sem=send, recv_sem=recv,
            device_id=where, device_id_type=MESH,
        )

    def landed(ref, sem):
        pltpu.make_async_copy(ref, ref, sem).wait()

    firsts = [
        pltpu.make_async_copy(a, b, s_own.at[i])
        for i, (a, b) in enumerate(
            [(raw, src), (gain, gn), (bias, bs), (idsin, ids), (wtin, wts)]
        )
    ]
    for copy in firsts:
        copy.start()
    barrier = pltpu.get_barrier_semaphore()
    for j in range(1, side):
        pl.semaphore_signal(
            barrier, inc=1, device_id={"ep": z * side + peer(j)}, device_id_type=MESH
        )
    for j in range(1, n):
        pl.semaphore_signal(barrier, inc=1, device_id=plane(j), device_id_type=MESH)
    pl.semaphore_signal(barrier, inc=1, device_id={"tp": 1 - core}, device_id_type=MESH)

    def send_tok(q, c, to, slot, way, kind):
        remote(
            tok.at[q, :, cols(c)], tok.at[slot, :, cols(c)],
            s_toks.at[way, kind], s_tok.at[slot, c], plane(to),
        ).start()

    def prep(q):
        ids0, ids1 = met[q, 0:1, :], met[q, 1:2, :]
        wt0, wt1 = met[q, 2:3, :], met[q, 3:4, :]
        row = lax.broadcasted_iota(jnp.int32, (rows, tokens), 0)
        e_row = (z * side + row // cap).astype(jnp.float32)
        s_row = lax.rem(row, cap).astype(jnp.float32)
        hit0 = (ids0 == e_row).astype(jnp.float32)
        hit1 = (ids1 == e_row).astype(jnp.float32)
        hit = hit0 + hit1
        before = (
            lax.broadcasted_iota(jnp.int32, (tokens, tokens), 0)
            < lax.broadcasted_iota(jnp.int32, (tokens, tokens), 1)
        ).astype(jnp.float32).astype(jnp.bfloat16)
        count = jnp.dot(hit.astype(jnp.bfloat16), before, preferred_element_type=jnp.float32)
        pick = jnp.where(count == s_row, hit, 0.0)
        sel[q] = pick.astype(jnp.bfloat16)
        w = pick * (hit0 * wt0 + hit1 * wt1)
        high = w.astype(jnp.bfloat16)
        mix[q, 0] = high
        mix[q, 1] = (w - high.astype(jnp.float32)).astype(jnp.bfloat16)

    for copy in firsts[3:]:
        copy.wait()
    met[0, 0:2, :] = ids[...].astype(jnp.float32)
    met[0, 2:4, :] = wts[...]
    met[0, 4:8, :] = jnp.zeros((4, tokens), jnp.float32)
    prep(0)
    for copy in firsts[:3]:
        copy.wait()
    slab = min(32, tokens)

    @pl.loop(0, tokens // slab)
    def _(i):
        at = pl.ds(pl.multiple_of(i * slab, slab), slab)
        v = src[at, :].astype(jnp.float32)
        v = v - jnp.mean(v, axis=-1, keepdims=True)
        spread = jnp.mean(v * v, axis=-1, keepdims=True)
        y = v * lax.rsqrt(spread + 1e-05) * gn[...] + bs[...]
        tok[0, at, :] = y.astype(jnp.bfloat16)

    pl.semaphore_wait(barrier, side - 1 + n)

    @pl.loop(0, k)
    def _(c):
        send_tok(0, c, up, 2, 0, 0)
        send_tok(0, c, back, 1, 1, 0)

    for i, (to, slot) in enumerate([(up, 2), (back, 1), (over, 3)]):
        remote(met.at[0], met.at[slot], s_mets.at[i], s_met.at[slot], plane(to)).start()

    def disp(q, c):
        y = jnp.dot(sel[q], tok[q, :, cols(c)], preferred_element_type=jnp.float32)
        snd[q, :, cols(c)] = y.astype(jnp.bfloat16)
        xin[q, band(p), cols(c)] = snd[q, band(p), cols(c)]
        for j in range(1, side):
            o = peer(j)
            remote(
                snd.at[q, band(o), cols(c)], xin.at[q, band(p), cols(c)],
                s_xs.at[q], s_x.at[q], {"ep": z * side + o},
            ).start()

    def others(ref, q):
        return ref.at[q, pl.ds(0, (side - 1) * cap)]

    tile = min(256, half)
    per = half // tile

    def gate(q, i):
        h, at = i // per, lax.rem(i, per)
        part = pl.ds(pl.multiple_of(at * tile, tile), tile)
        x = xin[q]
        g = jnp.dot(x, wg[h, :, part], preferred_element_type=jnp.float32)
        u = jnp.dot(x, wu[h, :, part], preferred_element_type=jnp.float32)
        v = g / (1.0 + jnp.exp(-g)) * u
        hid[q, :, pl.ds(pl.multiple_of(i * tile, tile), tile)] = v.astype(jnp.bfloat16)

    def gates(q):
        landed(others(xin, q), s_x.at[q])
        pl.loop(0, 2 * per)(lambda i: gate(q, i))

    def product(q, c):
        y = jnp.dot(hid[q], wd[:, cols(c)], preferred_element_type=jnp.float32)
        res[q, :, cols(c)] = y.astype(jnp.bfloat16)
        ret[q, band(p), cols(c)] = res[q, band(p), cols(c)]

    def give(q, c):
        for j in range(1, side):
            o = peer(j)
            remote(
                res.at[q, band(o), cols(c)], ret.at[q, band(p), cols(c)],
                s_rs.at[q], s_r.at[q, c], {"ep": z * side + o},
            ).start()

    def down(q, c):
        product(q, c)
        give(q, c)

    def weigh(q, c):
        landed(ret.at[q, pl.ds(0, (side - 1) * cap), cols(c)], s_r.at[q, c])
        r = ret[q, :, cols(c)]
        dims = (((0,), (0,)), ((), ()))
        return lax.dot_general(
            mix[q, 0], r, dims, preferred_element_type=jnp.float32
        ) + lax.dot_general(mix[q, 1], r, dims, preferred_element_type=jnp.float32)

    def combine(q, c, to, slot, add):
        y = weigh(q, c)
        if add:
            landed(racc.at[2, c], s_p.at[2, c])
            y = y + racc[2, c].astype(jnp.float32)
        psend[q - 1, c] = y.astype(jnp.bfloat16)
        remote(
            psend.at[q - 1, c], racc.at[slot, c], s_ps.at[q - 1], s_p.at[slot, c], plane(to)
        ).start()

    def arrived(q, c):
        landed(tok.at[q, :, cols(c)], s_tok.at[q, c])

    halfrows = pl.ds(pl.multiple_of(core * half, half), half)
    pairs = [
        (gw.at[0], wg.at[core]), (uw.at[0], wu.at[core]), (dw.at[0], wd.at[halfrows]),
    ]

    disp(0, 0)
    for i, (a, b) in enumerate(pairs):
        pltpu.make_async_copy(a, b, s_wl.at[i]).start()
        remote(a, b, s_ws.at[i], s_wr.at[i], {"tp": 1 - core}).start()
    pl.loop(1, k)(lambda c: disp(0, c))

    for q in (1, 2, 3):
        landed(met.at[q], s_met.at[q])
        prep(q)

    @pl.loop(0, HALF)
    def _(c):
        arrived(1, c)
        disp(1, c)
        arrived(2, c)
        send_tok(2, c, up, 3, 0, 1)
        disp(2, c)

    @pl.loop(HALF, k)
    def _(c):
        arrived(1, c)
        send_tok(1, c, back, 3, 1, 1)
        disp(1, c)
        arrived(2, c)
        disp(2, c)

    for i, (a, b) in enumerate(pairs):
        pltpu.make_async_copy(a, b, s_wl.at[i]).wait()
        landed(b, s_wr.at[i])
    landed(others(xin, 0), s_x.at[0])

    turns = 2 * per // HALF if 2 * per >= HALF else 1

    @pl.loop(0, HALF)
    def _(i):
        for c in (i, i + HALF):
            arrived(3, c)
            disp(3, c)
        for j in range(turns):
            gate(0, i * turns + j)

    pl.loop(0, k)(lambda c: product(0, c))
    gates(1)
    pl.loop(HALF, k)(lambda c: down(1, c))
    gates(2)
    pl.loop(0, HALF)(lambda c: down(2, c))
    gates(3)

    @pl.loop(0, HALF)
    def _(i):
        down(3, i)
        down(3, i + HALF)

    @pl.loop(0, HALF)
    def _(i):
        down(1, i)
        down(2, i + HALF)

    pl.loop(0, k)(lambda c: give(0, c))

    @pl.loop(0, HALF)
    def _(i):
        combine(1, i + HALF, up, 0, False)
        combine(2, i, back, 1, False)

    @pl.loop(0, HALF)
    def _(i):
        combine(3, i, up, 2, False)
        combine(3, i + HALF, back, 2, False)

    @pl.loop(0, HALF)
    def _(i):
        combine(1, i, up, 0, True)
        combine(2, i + HALF, back, 1, True)

    @pl.loop(0, k)
    def _(c):
        y = weigh(0, c)
        for slot in (0, 1):
            landed(racc.at[slot, c], s_p.at[slot, c])
            y = y + racc[slot, c].astype(jnp.float32)
        fin[:, cols(c)] = y.astype(out.dtype)
        pltpu.make_async_copy(fin.at[:, cols(c)], out.at[:, cols(c)], s_o.at[0]).start()

    for i, slot in enumerate((2, 1, 3)):
        landed(met.at[slot], s_mets.at[i])
    for i, (a, b) in enumerate(pairs):
        landed(b, s_ws.at[i])
    for way in range(2):
        landed(tok.at[0], s_toks.at[way, 0])
        landed(tok.at[0, :, pl.ds(0, HALF * wide)], s_toks.at[way, 1])
    for q in range(n):
        landed(others(snd, q), s_xs.at[q])
        landed(others(res, q), s_rs.at[q])
    for q in range(1, n):
        landed(psend.at[q - 1], s_ps.at[q - 1])
    pltpu.make_async_copy(fin, out, s_o.at[0]).wait()


def body(
    tokens, norm_gain, norm_bias, gate_weight, up_weight, down_weight, expert_ids, route_weights
):
    count, width = tokens.shape
    experts = lax.axis_size("ep")
    cap = max(4 * count // experts, 4)
    side = experts // LINE
    half = gate_weight.shape[2]
    rows = side * cap
    wide = width // CHUNKS
    bf = jnp.bfloat16
    dma = pltpu.SemaphoreType.DMA
    hbm = pl.BlockSpec(memory_space=pl.ANY)
    return pl.pallas_call(
        functools.partial(kernel, side),
        out_shape=jax.ShapeDtypeStruct((count, width), bf),
        in_specs=[hbm] * 8,
        out_specs=hbm,
        scratch_shapes=[
            pltpu.VMEM((count, width), bf),
            pltpu.VMEM((1, width), jnp.float32),
            pltpu.VMEM((1, width), jnp.float32),
            pltpu.VMEM((2, count), jnp.int32),
            pltpu.VMEM((2, count), jnp.float32),
            pltpu.VMEM((LINE, count, width), bf),
            pltpu.VMEM((LINE, 8, count), jnp.float32),
            pltpu.VMEM((2, width, half), bf),
            pltpu.VMEM((2, width, half), bf),
            pltpu.VMEM((2 * half, width), bf),
            pltpu.VMEM((LINE, rows, count), bf),
            pltpu.VMEM((LINE, 2, rows, count), bf),
            pltpu.VMEM((LINE, rows, width), bf),
            pltpu.VMEM((LINE, rows, width), bf),
            pltpu.VMEM((LINE, rows, 2 * half), bf),
            pltpu.VMEM((LINE, rows, width), bf),
            pltpu.VMEM((LINE, rows, width), bf),
            pltpu.VMEM((LINE - 1, CHUNKS, count, wide), bf),
            pltpu.VMEM((LINE - 1, CHUNKS, count, wide), bf),
            pltpu.VMEM((count, width), bf),
            dma((5,)),
            dma((LINE,)),
            dma((LINE - 1,)),
            dma((3,)),
            dma((3,)),
            dma((3,)),
            dma((LINE, CHUNKS)),
            dma((2, 2)),
            dma((LINE,)),
            dma((LINE,)),
            dma((LINE, CHUNKS)),
            dma((LINE,)),
            dma((LINE - 1, CHUNKS)),
            dma((LINE - 1,)),
            dma((1,)),
        ],
        compiler_params=pltpu.CompilerParams(
            collective_id=0, has_side_effects=True, vmem_limit_bytes=60 * 1024 * 1024
        ),
    )(
        tokens, norm_gain[None], norm_bias[None], expert_ids.T, route_weights.T,
        gate_weight, up_weight, down_weight,
    )


def solution(mesh):
    placed = (
        P(("ep", "tp"), None),
        P(),
        P(),
        P("ep", None, "tp"),
        P("ep", None, "tp"),
        P("ep", "tp", None),
        P(("ep", "tp"), None),
        P(("ep", "tp"), None),
    )
    return jax.shard_map(
        body, mesh=mesh, in_specs=placed, out_specs=P(("ep", "tp"), None), check_vma=False
    )
```

```python
import functools

import jax
import jax.numpy as jnp
from jax import lax
from jax.experimental import pallas as pl
from jax.experimental.pallas import tpu as pltpu
from jax.sharding import PartitionSpec as P

MESH = pl.DeviceIdType.MESH
LINE = 4
CHUNKS = 8
HALF = CHUNKS // 2


def kernel(
    planes, raw, gain, bias, idsin, wtin, gw, uw, dw, out,
    src, gn, bs, mu, rs, ids, wts, tok, met, wg, wu, wd, sel, mix, snd, xin, hid, res, ret, psend, racc,
    fin, s_own, s_met, s_mets, s_wl, s_ws, s_wr, s_tok, s_toks, s_x, s_xs, s_r, s_rs, s_p, s_ps, s_o,
):
    n = LINE
    side = planes
    me, core = lax.axis_index("ep"), lax.axis_index("tp")
    z, p = me // side, lax.rem(me, side)
    tokens, width = raw.shape
    half = gw.shape[2]
    rows = snd.shape[1]
    cap = rows // side
    k = CHUNKS
    wide = width // k

    def cols(c):
        return pl.ds(pl.multiple_of(c * wide, wide), wide)

    def band(i):
        return pl.ds(pl.multiple_of(i * cap, cap), cap)

    def plane(j):
        return {"ep": lax.rem(z + j, n) * side + p}

    up, over, back = 1, 2, n - 1

    def peer(j):
        return lax.rem(p + j, side)

    def remote(src, dst, send, recv, where):
        return pltpu.make_async_remote_copy(
            src_ref=src, dst_ref=dst, send_sem=send, recv_sem=recv,
            device_id=where, device_id_type=MESH,
        )

    def landed(ref, sem):
        pltpu.make_async_copy(ref, ref, sem).wait()

    def step(name):
        def run(f):
            with jax.named_scope(name):
                f()
        return run

    firsts = [
        pltpu.make_async_copy(a, b, s_own.at[i])
        for i, (a, b) in enumerate(
            [(raw, src), (gain, gn), (bias, bs), (idsin, ids), (wtin, wts)]
        )
    ]
    for copy in firsts:
        copy.start()
    barrier = pltpu.get_barrier_semaphore()
    for j in range(1, side):
        pl.semaphore_signal(
            barrier, inc=1, device_id={"ep": z * side + peer(j)}, device_id_type=MESH
        )
    for j in range(1, n):
        pl.semaphore_signal(barrier, inc=1, device_id=plane(j), device_id_type=MESH)
    pl.semaphore_signal(barrier, inc=1, device_id={"tp": 1 - core}, device_id_type=MESH)

    def send_tok(q, c, to, slot, way, kind):
        remote(
            tok.at[q, :, cols(c)], tok.at[slot, :, cols(c)],
            s_toks.at[way, kind], s_tok.at[slot, c], plane(to),
        ).start()

    def prep(q):
        ids0, ids1 = met[q, 0:1, :], met[q, 1:2, :]
        wt0, wt1 = met[q, 2:3, :], met[q, 3:4, :]
        row = lax.broadcasted_iota(jnp.int32, (rows, tokens), 0)
        e_row = (z * side + row // cap).astype(jnp.float32)
        s_row = lax.rem(row, cap).astype(jnp.float32)
        hit0 = (ids0 == e_row).astype(jnp.float32)
        hit1 = (ids1 == e_row).astype(jnp.float32)
        hit = hit0 + hit1
        before = (
            lax.broadcasted_iota(jnp.int32, (tokens, tokens), 0)
            < lax.broadcasted_iota(jnp.int32, (tokens, tokens), 1)
        ).astype(jnp.float32).astype(jnp.bfloat16)
        count = jnp.dot(hit.astype(jnp.bfloat16), before, preferred_element_type=jnp.float32)
        pick = jnp.where(count == s_row, hit, 0.0)
        sel[q] = pick.astype(jnp.bfloat16)
        w = pick * (hit0 * wt0 + hit1 * wt1)
        high = w.astype(jnp.bfloat16)
        mix[q, 0] = high
        mix[q, 1] = (w - high.astype(jnp.float32)).astype(jnp.bfloat16)

    @step("prep0")
    def _():
        for copy in firsts[3:]:
            copy.wait()
        met[0, 0:2, :] = ids[...].astype(jnp.float32)
        met[0, 2:4, :] = wts[...]
        met[0, 4:8, :] = jnp.zeros((4, tokens), jnp.float32)
        prep(0)

    @step("raw")
    def _():
        for copy in firsts[:3]:
            copy.wait()

    slab = min(32, tokens)

    @step("stats")
    def _():
        @pl.loop(0, tokens // slab)
        def _(i):
            at = pl.ds(pl.multiple_of(i * slab, slab), slab)
            v = src[at, :].astype(jnp.float32)
            mean = jnp.mean(v, axis=-1, keepdims=True)
            v = v - mean
            spread = jnp.mean(v * v, axis=-1, keepdims=True)
            mu[at, :] = mean
            rs[at, :] = lax.rsqrt(spread + 1e-05)

    @step("meet")
    def _():
        pl.semaphore_wait(barrier, side - 1 + n)

    @step("own")
    def _():
        for i, (to, slot) in enumerate([(up, 2), (back, 1), (over, 3)]):
            remote(met.at[0], met.at[slot], s_mets.at[i], s_met.at[slot], plane(to)).start()

    def disp(q, c):
        y = jnp.dot(sel[q], tok[q, :, cols(c)], preferred_element_type=jnp.float32)
        snd[q, :, cols(c)] = y.astype(jnp.bfloat16)
        xin[q, band(p), cols(c)] = snd[q, band(p), cols(c)]
        for j in range(1, side):
            o = peer(j)
            remote(
                snd.at[q, band(o), cols(c)], xin.at[q, band(p), cols(c)],
                s_xs.at[q], s_x.at[q], {"ep": z * side + o},
            ).start()

    def others(ref, q):
        return ref.at[q, pl.ds(0, (side - 1) * cap)]

    tile = min(256, half)
    per = half // tile

    def gate(q, i):
        h, at = i // per, lax.rem(i, per)
        part = pl.ds(pl.multiple_of(at * tile, tile), tile)
        x = xin[q]
        g = jnp.dot(x, wg[h, :, part], preferred_element_type=jnp.float32)
        u = jnp.dot(x, wu[h, :, part], preferred_element_type=jnp.float32)
        v = g / (1.0 + jnp.exp(-g)) * u
        hid[q, :, pl.ds(pl.multiple_of(i * tile, tile), tile)] = v.astype(jnp.bfloat16)

    def gates(q):
        pl.loop(0, 2 * per)(lambda i: gate(q, i))

    def product(q, c):
        y = jnp.dot(hid[q], wd[:, cols(c)], preferred_element_type=jnp.float32)
        res[q, :, cols(c)] = y.astype(jnp.bfloat16)
        ret[q, band(p), cols(c)] = res[q, band(p), cols(c)]

    def give(q, c):
        for j in range(1, side):
            o = peer(j)
            remote(
                res.at[q, band(o), cols(c)], ret.at[q, band(p), cols(c)],
                s_rs.at[q], s_r.at[q, c], {"ep": z * side + o},
            ).start()

    def down(q, c):
        product(q, c)
        give(q, c)

    def weigh(q, c):
        r = ret[q, :, cols(c)]
        dims = (((0,), (0,)), ((), ()))
        return lax.dot_general(
            mix[q, 0], r, dims, preferred_element_type=jnp.float32
        ) + lax.dot_general(mix[q, 1], r, dims, preferred_element_type=jnp.float32)

    def combine(q, c, to, slot, add):
        landed(ret.at[q, pl.ds(0, (side - 1) * cap), cols(c)], s_r.at[q, c])
        y = weigh(q, c)
        if add:
            landed(racc.at[2, c], s_p.at[2, c])
            y = y + racc[2, c].astype(jnp.float32)
        psend[q - 1, c] = y.astype(jnp.bfloat16)
        remote(
            psend.at[q - 1, c], racc.at[slot, c], s_ps.at[q - 1], s_p.at[slot, c], plane(to)
        ).start()

    def arrived(q, c):
        landed(tok.at[q, :, cols(c)], s_tok.at[q, c])

    halfrows = pl.ds(pl.multiple_of(core * half, half), half)
    pairs = [
        (gw.at[0], wg.at[core]), (uw.at[0], wu.at[core]), (dw.at[0], wd.at[halfrows]),
    ]

    def first(c):
        v = (src[:, cols(c)].astype(jnp.float32) - mu[...]) * rs[...]
        tok[0, :, cols(c)] = (v * gn[:, cols(c)] + bs[:, cols(c)]).astype(jnp.bfloat16)
        send_tok(0, c, up, 2, 0, 0)
        send_tok(0, c, back, 1, 1, 0)
        disp(0, c)

    @step("disp0")
    def _():
        first(0)
        for i, (a, b) in enumerate(pairs):
            pltpu.make_async_copy(a, b, s_wl.at[i]).start()
            remote(a, b, s_ws.at[i], s_wr.at[i], {"tp": 1 - core}).start()
        pl.loop(1, k)(first)

    @step("preps")
    def _():
        for q in (1, 2, 3):
            landed(met.at[q], s_met.at[q])
            prep(q)

    @step("disp12a")
    def _():
        @pl.loop(0, HALF)
        def _(c):
            arrived(1, c)
            disp(1, c)
            arrived(2, c)
            send_tok(2, c, up, 3, 0, 1)
            disp(2, c)

    @step("disp12b")
    def _():
        @pl.loop(HALF, k)
        def _(c):
            arrived(1, c)
            send_tok(1, c, back, 3, 1, 1)
            disp(1, c)
            arrived(2, c)
            disp(2, c)

    @step("weights")
    def _():
        for i, (a, b) in enumerate(pairs):
            pltpu.make_async_copy(a, b, s_wl.at[i]).wait()
            landed(b, s_wr.at[i])

    @step("in0")
    def _():
        landed(others(xin, 0), s_x.at[0])

    turns = 2 * per // HALF if 2 * per >= HALF else 1

    @step("disp3gate0")
    def _():
        @pl.loop(0, HALF)
        def _(i):
            for c in (i, i + HALF):
                arrived(3, c)
                disp(3, c)
            for j in range(turns):
                gate(0, i * turns + j)

    @step("product0")
    def _():
        pl.loop(0, k)(lambda c: product(0, c))

    @step("in1")
    def _():
        landed(others(xin, 1), s_x.at[1])

    @step("gates1")
    def _():
        gates(1)

    @step("down1")
    def _():
        pl.loop(HALF, k)(lambda c: down(1, c))

    @step("in2")
    def _():
        landed(others(xin, 2), s_x.at[2])

    @step("gates2")
    def _():
        gates(2)

    @step("down2")
    def _():
        pl.loop(0, HALF)(lambda c: down(2, c))

    @step("in3")
    def _():
        landed(others(xin, 3), s_x.at[3])

    @step("gates3")
    def _():
        gates(3)

    @step("down3")
    def _():
        @pl.loop(0, HALF)
        def _(i):
            down(3, i)
            down(3, i + HALF)
            combine(1, i + HALF, up, 0, False)
            combine(2, i, back, 1, False)

    @step("down12")
    def _():
        @pl.loop(0, HALF)
        def _(i):
            down(1, i)
            down(2, i + HALF)

    @step("give0")
    def _():
        pl.loop(0, k)(lambda c: give(0, c))

    @step("comb3")
    def _():
        @pl.loop(0, HALF)
        def _(i):
            combine(3, i, up, 2, False)
            combine(3, i + HALF, back, 2, False)

    @step("comb12b")
    def _():
        @pl.loop(0, HALF)
        def _(i):
            combine(1, i, up, 0, True)
            combine(2, i + HALF, back, 1, True)

    @step("last")
    def _():
        @pl.loop(0, k)
        def _(c):
            with jax.named_scope("wr"):
                landed(ret.at[0, pl.ds(0, (side - 1) * cap), cols(c)], s_r.at[0, c])
            with jax.named_scope("wp"):
                for slot in (0, 1):
                    landed(racc.at[slot, c], s_p.at[slot, c])
            y = weigh(0, c)
            for slot in (0, 1):
                y = y + racc[slot, c].astype(jnp.float32)
            fin[:, cols(c)] = y.astype(out.dtype)
            pltpu.make_async_copy(fin.at[:, cols(c)], out.at[:, cols(c)], s_o.at[0]).start()

    for i, slot in enumerate((2, 1, 3)):
        landed(met.at[slot], s_mets.at[i])
    for i, (a, b) in enumerate(pairs):
        landed(b, s_ws.at[i])
    for way in range(2):
        landed(tok.at[0], s_toks.at[way, 0])
        landed(tok.at[0, :, pl.ds(0, HALF * wide)], s_toks.at[way, 1])
    for q in range(n):
        landed(others(snd, q), s_xs.at[q])
        landed(others(res, q), s_rs.at[q])
    for q in range(1, n):
        landed(psend.at[q - 1], s_ps.at[q - 1])
    pltpu.make_async_copy(fin, out, s_o.at[0]).wait()


def body(
    tokens, norm_gain, norm_bias, gate_weight, up_weight, down_weight, expert_ids, route_weights
):
    count, width = tokens.shape
    experts = lax.axis_size("ep")
    cap = max(4 * count // experts, 4)
    side = experts // LINE
    half = gate_weight.shape[2]
    rows = side * cap
    wide = width // CHUNKS
    bf = jnp.bfloat16
    dma = pltpu.SemaphoreType.DMA
    hbm = pl.BlockSpec(memory_space=pl.ANY)
    return pl.pallas_call(
        functools.partial(kernel, side),
        out_shape=jax.ShapeDtypeStruct((count, width), bf),
        in_specs=[hbm] * 8,
        out_specs=hbm,
        scratch_shapes=[
            pltpu.VMEM((count, width), bf),
            pltpu.VMEM((1, width), jnp.float32),
            pltpu.VMEM((1, width), jnp.float32),
            pltpu.VMEM((count, 1), jnp.float32),
            pltpu.VMEM((count, 1), jnp.float32),
            pltpu.VMEM((2, count), jnp.int32),
            pltpu.VMEM((2, count), jnp.float32),
            pltpu.VMEM((LINE, count, width), bf),
            pltpu.VMEM((LINE, 8, count), jnp.float32),
            pltpu.VMEM((2, width, half), bf),
            pltpu.VMEM((2, width, half), bf),
            pltpu.VMEM((2 * half, width), bf),
            pltpu.VMEM((LINE, rows, count), bf),
            pltpu.VMEM((LINE, 2, rows, count), bf),
            pltpu.VMEM((LINE, rows, width), bf),
            pltpu.VMEM((LINE, rows, width), bf),
            pltpu.VMEM((LINE, rows, 2 * half), bf),
            pltpu.VMEM((LINE, rows, width), bf),
            pltpu.VMEM((LINE, rows, width), bf),
            pltpu.VMEM((LINE - 1, CHUNKS, count, wide), bf),
            pltpu.VMEM((LINE - 1, CHUNKS, count, wide), bf),
            pltpu.VMEM((count, width), bf),
            dma((5,)),
            dma((LINE,)),
            dma((LINE - 1,)),
            dma((3,)),
            dma((3,)),
            dma((3,)),
            dma((LINE, CHUNKS)),
            dma((2, 2)),
            dma((LINE,)),
            dma((LINE,)),
            dma((LINE, CHUNKS)),
            dma((LINE,)),
            dma((LINE - 1, CHUNKS)),
            dma((LINE - 1,)),
            dma((1,)),
        ],
        compiler_params=pltpu.CompilerParams(
            collective_id=0, has_side_effects=True, vmem_limit_bytes=60 * 1024 * 1024
        ),
    )(
        tokens, norm_gain[None], norm_bias[None], expert_ids.T, route_weights.T,
        gate_weight, up_weight, down_weight,
    )


def solution(mesh):
    placed = (
        P(("ep", "tp"), None),
        P(),
        P(),
        P("ep", None, "tp"),
        P("ep", None, "tp"),
        P("ep", "tp", None),
        P(("ep", "tp"), None),
        P(("ep", "tp"), None),
    )
    return jax.shard_map(
        body, mesh=mesh, in_specs=placed, out_specs=P(("ep", "tp"), None), check_vma=False
    )
```

```python
import functools

import jax
import jax.numpy as jnp
from jax import lax
from jax.experimental import pallas as pl
from jax.experimental.pallas import tpu as pltpu
from jax.sharding import PartitionSpec as P

MESH = pl.DeviceIdType.MESH
LINE = 4
CHUNKS = 8
HALF = CHUNKS // 2


def kernel(
    planes, raw, gain, bias, idsin, wtin, gw, uw, dw, out,
    src, gn, bs, part, mu, rs, ids, wts, tok, met, wg, wu, wd, sel, mix, snd, xin, hid, res, ret, psend, racc,
    s_own, s_met, s_mets, s_wl, s_ws, s_wr, s_tok, s_toks, s_x, s_xs, s_r, s_rs, s_p, s_ps,
):
    n = LINE
    side = planes
    me, core = lax.axis_index("ep"), lax.axis_index("tp")
    z, p = me // side, lax.rem(me, side)
    tokens, width = raw.shape
    half = gw.shape[2]
    rows = snd.shape[1]
    cap = rows // side
    k = CHUNKS
    wide = width // k

    def cols(c):
        return pl.ds(pl.multiple_of(c * wide, wide), wide)

    def band(i):
        return pl.ds(pl.multiple_of(i * cap, cap), cap)

    def plane(j):
        return {"ep": lax.rem(z + j, n) * side + p}

    up, over, back = 1, 2, n - 1

    def peer(j):
        return lax.rem(p + j, side)

    def remote(src, dst, send, recv, where):
        return pltpu.make_async_remote_copy(
            src_ref=src, dst_ref=dst, send_sem=send, recv_sem=recv,
            device_id=where, device_id_type=MESH,
        )

    def landed(ref, sem):
        pltpu.make_async_copy(ref, ref, sem).wait()

    def step(name):
        def run(f):
            with jax.named_scope(name):
                f()
        return run

    firsts = [
        pltpu.make_async_copy(a, b, s_own.at[i])
        for i, (a, b) in enumerate(
            [(raw, src), (gain, gn), (bias, bs), (idsin, ids), (wtin, wts)]
        )
    ]
    for copy in firsts:
        copy.start()
    barrier = pltpu.get_barrier_semaphore()
    for j in range(1, side):
        pl.semaphore_signal(
            barrier, inc=1, device_id={"ep": z * side + peer(j)}, device_id_type=MESH
        )
    for j in range(1, n):
        pl.semaphore_signal(barrier, inc=1, device_id=plane(j), device_id_type=MESH)
    pl.semaphore_signal(barrier, inc=1, device_id={"tp": 1 - core}, device_id_type=MESH)

    def send_tok(q, c, to, slot, way, kind):
        remote(
            tok.at[q, :, cols(c)], tok.at[slot, :, cols(c)],
            s_toks.at[way, kind], s_tok.at[slot, c], plane(to),
        ).start()

    def prep(q):
        ids0, ids1 = met[q, 0:1, :], met[q, 1:2, :]
        wt0, wt1 = met[q, 2:3, :], met[q, 3:4, :]
        row = lax.broadcasted_iota(jnp.int32, (rows, tokens), 0)
        e_row = (z * side + row // cap).astype(jnp.float32)
        s_row = lax.rem(row, cap).astype(jnp.float32)
        hit0 = (ids0 == e_row).astype(jnp.float32)
        hit1 = (ids1 == e_row).astype(jnp.float32)
        hit = hit0 + hit1
        before = (
            lax.broadcasted_iota(jnp.int32, (tokens, tokens), 0)
            < lax.broadcasted_iota(jnp.int32, (tokens, tokens), 1)
        ).astype(jnp.float32).astype(jnp.bfloat16)
        count = jnp.dot(hit.astype(jnp.bfloat16), before, preferred_element_type=jnp.float32)
        pick = jnp.where(count == s_row, hit, 0.0)
        sel[q] = pick.astype(jnp.bfloat16)
        w = pick * (hit0 * wt0 + hit1 * wt1)
        high = w.astype(jnp.bfloat16)
        mix[q, 0] = high
        mix[q, 1] = (w - high.astype(jnp.float32)).astype(jnp.bfloat16)

    @step("prep0")
    def _():
        for copy in firsts[3:]:
            copy.wait()
        met[0, 0:2, :] = ids[...].astype(jnp.float32)
        met[0, 2:4, :] = wts[...]
        met[0, 4:8, :] = jnp.zeros((4, tokens), jnp.float32)
        prep(0)

    @step("raw")
    def _():
        for copy in firsts[:3]:
            copy.wait()

    slab = min(32, tokens)
    lanes = part.shape[1]

    @step("stats")
    def _():
        def total(i, f):
            at = pl.ds(pl.multiple_of(i * slab, slab), slab)
            parts = [
                f(src[at, j * lanes : (j + 1) * lanes].astype(jnp.float32), at)
                for j in range(width // lanes)
            ]
            while len(parts) > 1:
                parts = [a + b for a, b in zip(parts[::2], parts[1::2])]
            part[at, :] = parts[0]

        pl.loop(0, tokens // slab)(lambda i: total(i, lambda v, at: v))
        mu[...] = jnp.sum(part[...], axis=-1, keepdims=True) / width

        def square(v, at):
            v = v - mu[at, :]
            return v * v

        pl.loop(0, tokens // slab)(lambda i: total(i, square))
        rs[...] = lax.rsqrt(jnp.sum(part[...], axis=-1, keepdims=True) / width + 1e-05)

    @step("meet")
    def _():
        pl.semaphore_wait(barrier, side - 1 + n)

    @step("own")
    def _():
        for i, (to, slot) in enumerate([(up, 2), (back, 1), (over, 3)]):
            remote(met.at[0], met.at[slot], s_mets.at[i], s_met.at[slot], plane(to)).start()

    def disp(q, c):
        y = jnp.dot(sel[q], tok[q, :, cols(c)], preferred_element_type=jnp.float32)
        snd[q, :, cols(c)] = y.astype(jnp.bfloat16)
        xin[q, band(p), cols(c)] = snd[q, band(p), cols(c)]
        for j in range(1, side):
            o = peer(j)
            remote(
                snd.at[q, band(o), cols(c)], xin.at[q, band(p), cols(c)],
                s_xs.at[q], s_x.at[q], {"ep": z * side + o},
            ).start()

    def others(ref, q):
        return ref.at[q, pl.ds(0, (side - 1) * cap)]

    tile = min(256, half)
    per = half // tile

    def gate(q, i):
        h, at = i // per, lax.rem(i, per)
        part = pl.ds(pl.multiple_of(at * tile, tile), tile)
        x = xin[q]
        g = jnp.dot(x, wg[h, :, part], preferred_element_type=jnp.float32)
        u = jnp.dot(x, wu[h, :, part], preferred_element_type=jnp.float32)
        v = g / (1.0 + jnp.exp(-g)) * u
        hid[q, :, pl.ds(pl.multiple_of(i * tile, tile), tile)] = v.astype(jnp.bfloat16)

    def gates(q):
        pl.loop(0, 2 * per)(lambda i: gate(q, i))

    def product(q, c):
        y = jnp.dot(hid[q], wd[:, cols(c)], preferred_element_type=jnp.float32)
        res[q, :, cols(c)] = y.astype(jnp.bfloat16)
        ret[q, band(p), cols(c)] = res[q, band(p), cols(c)]

    def give(q, c):
        for j in range(1, side):
            o = peer(j)
            remote(
                res.at[q, band(o), cols(c)], ret.at[q, band(p), cols(c)],
                s_rs.at[q], s_r.at[q, c], {"ep": z * side + o},
            ).start()

    def down(q, c):
        product(q, c)
        give(q, c)

    def weigh(q, c):
        r = ret[q, :, cols(c)]
        dims = (((0,), (0,)), ((), ()))
        return lax.dot_general(
            mix[q, 0], r, dims, preferred_element_type=jnp.float32
        ) + lax.dot_general(mix[q, 1], r, dims, preferred_element_type=jnp.float32)

    def combine(q, c, to, slot, add):
        landed(ret.at[q, pl.ds(0, (side - 1) * cap), cols(c)], s_r.at[q, c])
        y = weigh(q, c)
        if add:
            landed(racc.at[2, c], s_p.at[2, c])
            y = y + racc[2, c].astype(jnp.float32)
        psend[q - 1, c] = y.astype(jnp.bfloat16)
        remote(
            psend.at[q - 1, c], racc.at[slot, c], s_ps.at[q - 1], s_p.at[slot, c], plane(to)
        ).start()

    def arrived(q, c):
        landed(tok.at[q, :, cols(c)], s_tok.at[q, c])

    halfrows = pl.ds(pl.multiple_of(core * half, half), half)
    pairs = [
        (gw.at[0], wg.at[core]), (uw.at[0], wu.at[core]), (dw.at[0], wd.at[halfrows]),
    ]

    def first(c):
        v = (src[:, cols(c)].astype(jnp.float32) - mu[...]) * rs[...]
        tok[0, :, cols(c)] = (v * gn[:, cols(c)] + bs[:, cols(c)]).astype(jnp.bfloat16)
        send_tok(0, c, up, 2, 0, 0)
        send_tok(0, c, back, 1, 1, 0)
        disp(0, c)

    @step("disp0")
    def _():
        first(0)
        for i, (a, b) in enumerate(pairs):
            pltpu.make_async_copy(a, b, s_wl.at[i]).start()
            remote(a, b, s_ws.at[i], s_wr.at[i], {"tp": 1 - core}).start()
        pl.loop(1, k)(first)

    @step("preps")
    def _():
        for q in (1, 2, 3):
            landed(met.at[q], s_met.at[q])
            prep(q)

    @step("disp12a")
    def _():
        @pl.loop(0, HALF)
        def _(c):
            arrived(1, c)
            disp(1, c)
            arrived(2, c)
            send_tok(2, c, up, 3, 0, 1)
            disp(2, c)

    @step("disp12b")
    def _():
        @pl.loop(HALF, k)
        def _(c):
            arrived(1, c)
            send_tok(1, c, back, 3, 1, 1)
            disp(1, c)
            arrived(2, c)
            disp(2, c)

    @step("weights")
    def _():
        for i, (a, b) in enumerate(pairs):
            pltpu.make_async_copy(a, b, s_wl.at[i]).wait()
            landed(b, s_wr.at[i])

    @step("in0")
    def _():
        landed(others(xin, 0), s_x.at[0])

    turns = 2 * per // HALF if 2 * per >= HALF else 1

    @step("disp3gate0")
    def _():
        @pl.loop(0, HALF)
        def _(i):
            for c in (i, i + HALF):
                arrived(3, c)
                disp(3, c)
            for j in range(turns):
                gate(0, i * turns + j)

    @step("product0")
    def _():
        pl.loop(0, k)(lambda c: product(0, c))

    @step("in1")
    def _():
        landed(others(xin, 1), s_x.at[1])

    @step("gates1")
    def _():
        gates(1)

    @step("down1")
    def _():
        pl.loop(HALF, k)(lambda c: down(1, c))

    @step("in2")
    def _():
        landed(others(xin, 2), s_x.at[2])

    @step("gates2")
    def _():
        gates(2)

    @step("down2")
    def _():
        pl.loop(0, HALF)(lambda c: down(2, c))

    @step("in3")
    def _():
        landed(others(xin, 3), s_x.at[3])

    @step("gates3")
    def _():
        gates(3)

    @step("down3")
    def _():
        @pl.loop(0, HALF)
        def _(i):
            down(3, i)
            down(3, i + HALF)
            combine(1, i + HALF, up, 0, False)
            combine(2, i, back, 1, False)

    @step("down12")
    def _():
        @pl.loop(0, HALF)
        def _(i):
            down(1, i)
            down(2, i + HALF)

    @step("give0")
    def _():
        pl.loop(0, k)(lambda c: give(0, c))

    @step("comb3")
    def _():
        @pl.loop(0, HALF)
        def _(i):
            combine(3, i, up, 2, False)
            combine(3, i + HALF, back, 2, False)

    @step("comb12b")
    def _():
        @pl.loop(0, HALF)
        def _(i):
            combine(1, i, up, 0, True)
            combine(2, i + HALF, back, 1, True)

    @step("drain")
    def _():
        for i, slot in enumerate((2, 1, 3)):
            landed(met.at[slot], s_mets.at[i])
        for i, (a, b) in enumerate(pairs):
            landed(b, s_ws.at[i])
        for way in range(2):
            landed(tok.at[0], s_toks.at[way, 0])
            landed(tok.at[0, :, pl.ds(0, HALF * wide)], s_toks.at[way, 1])
        for q in range(n):
            landed(others(snd, q), s_xs.at[q])
        for q in range(1, n):
            landed(others(res, q), s_rs.at[q])

    @step("last")
    def _():
        @pl.loop(0, k)
        def _(c):
            with jax.named_scope("wr"):
                landed(ret.at[0, pl.ds(0, (side - 1) * cap), cols(c)], s_r.at[0, c])
            with jax.named_scope("wp"):
                for slot in (0, 1):
                    landed(racc.at[slot, c], s_p.at[slot, c])
            y = weigh(0, c)
            for slot in (0, 1):
                y = y + racc[slot, c].astype(jnp.float32)
            out[:, cols(c)] = y.astype(out.dtype)

    @step("end")
    def _():
        for q in range(1, n):
            landed(psend.at[q - 1], s_ps.at[q - 1])
        landed(others(res, 0), s_rs.at[0])


def body(
    tokens, norm_gain, norm_bias, gate_weight, up_weight, down_weight, expert_ids, route_weights
):
    count, width = tokens.shape
    experts = lax.axis_size("ep")
    cap = max(4 * count // experts, 4)
    side = experts // LINE
    half = gate_weight.shape[2]
    rows = side * cap
    wide = width // CHUNKS
    bf = jnp.bfloat16
    dma = pltpu.SemaphoreType.DMA
    hbm = pl.BlockSpec(memory_space=pl.ANY)
    return pl.pallas_call(
        functools.partial(kernel, side),
        out_shape=pltpu.VMEM((count, width), bf),
        in_specs=[hbm] * 8,
        out_specs=pl.BlockSpec(memory_space=pltpu.VMEM),
        scratch_shapes=[
            pltpu.VMEM((count, width), bf),
            pltpu.VMEM((1, width), jnp.float32),
            pltpu.VMEM((1, width), jnp.float32),
            pltpu.VMEM((count, 128), jnp.float32),
            pltpu.VMEM((count, 1), jnp.float32),
            pltpu.VMEM((count, 1), jnp.float32),
            pltpu.VMEM((2, count), jnp.int32),
            pltpu.VMEM((2, count), jnp.float32),
            pltpu.VMEM((LINE, count, width), bf),
            pltpu.VMEM((LINE, 8, count), jnp.float32),
            pltpu.VMEM((2, width, half), bf),
            pltpu.VMEM((2, width, half), bf),
            pltpu.VMEM((2 * half, width), bf),
            pltpu.VMEM((LINE, rows, count), bf),
            pltpu.VMEM((LINE, 2, rows, count), bf),
            pltpu.VMEM((LINE, rows, width), bf),
            pltpu.VMEM((LINE, rows, width), bf),
            pltpu.VMEM((LINE, rows, 2 * half), bf),
            pltpu.VMEM((LINE, rows, width), bf),
            pltpu.VMEM((LINE, rows, width), bf),
            pltpu.VMEM((LINE - 1, CHUNKS, count, wide), bf),
            pltpu.VMEM((LINE - 1, CHUNKS, count, wide), bf),
            dma((5,)),
            dma((LINE,)),
            dma((LINE - 1,)),
            dma((3,)),
            dma((3,)),
            dma((3,)),
            dma((LINE, CHUNKS)),
            dma((2, 2)),
            dma((LINE,)),
            dma((LINE,)),
            dma((LINE, CHUNKS)),
            dma((LINE,)),
            dma((LINE - 1, CHUNKS)),
            dma((LINE - 1,)),
        ],
        compiler_params=pltpu.CompilerParams(
            collective_id=0, has_side_effects=True, vmem_limit_bytes=52 * 1024 * 1024
        ),
    )(
        *[
            pltpu.with_memory_space_constraint(a, pltpu.HBM)
            for a in (
                tokens, norm_gain[None], norm_bias[None], expert_ids.T, route_weights.T,
                gate_weight, up_weight, down_weight,
            )
        ]
    )


def solution(mesh):
    placed = (
        P(("ep", "tp"), None),
        P(),
        P(),
        P("ep", None, "tp"),
        P("ep", None, "tp"),
        P("ep", "tp", None),
        P(("ep", "tp"), None),
        P(("ep", "tp"), None),
    )
    return jax.shard_map(
        body, mesh=mesh, in_specs=placed, out_specs=P(("ep", "tp"), None), check_vma=False
    )
```

```python
import functools

import jax
import jax.numpy as jnp
from jax import lax
from jax.experimental import pallas as pl
from jax.experimental.pallas import tpu as pltpu
from jax.sharding import PartitionSpec as P

MESH = pl.DeviceIdType.MESH
LINE = 4
CHUNKS = 8
HALF = CHUNKS // 2
EARLY = 2


def kernel(
    planes, raw, gain, bias, idsin, wtin, gw, uw, dw, out,
    src, gn, bs, part, mu, rs, ids, wts, tok, met, wg, wu, wd, sel, mix, snd, xin, hid, res, ret, psend, racc,
    s_own, s_met, s_w, s_ws, s_tok, s_toks, s_x, s_xs, s_r, s_rs, s_p, s_ps,
):
    n = LINE
    side = planes
    me, core = lax.axis_index("ep"), lax.axis_index("tp")
    z, p = me // side, lax.rem(me, side)
    tokens, width = raw.shape
    half = gw.shape[2]
    rows = snd.shape[1]
    cap = rows // side
    k = CHUNKS
    wide = width // k

    def cols(c):
        return pl.ds(pl.multiple_of(c * wide, wide), wide)

    def band(i):
        return pl.ds(pl.multiple_of(i * cap, cap), cap)

    def plane(j):
        return {"ep": lax.rem(z + j, n) * side + p}

    up, over, back = 1, 2, n - 1

    y, x = p // n, lax.rem(p, n)

    def away(d):
        return sum(min(j, n - j) for j in d)

    offsets = [(b, c) for b in range(n) for c in range(n) if b or c]
    peers = [
        lax.rem(y + b, n) * n + lax.rem(x + c, n)
        for b, c in sorted(offsets, key=lambda d: -away(d))
    ]

    def remote(src, dst, send, recv, where):
        return pltpu.make_async_remote_copy(
            src_ref=src, dst_ref=dst, send_sem=send, recv_sem=recv,
            device_id=where, device_id_type=MESH,
        )

    def landed(ref, sem):
        pltpu.make_async_copy(ref, ref, sem).wait()

    def step(name):
        def run(f):
            with jax.named_scope(name):
                f()
        return run

    firsts = [
        pltpu.make_async_copy(a, b, s_own.at[i])
        for i, (a, b) in enumerate(
            [(raw, src), (gain, gn), (bias, bs), (idsin, ids), (wtin, wts)]
        )
    ]
    for copy in firsts:
        copy.start()
    barrier = pltpu.get_barrier_semaphore()
    for o in peers:
        pl.semaphore_signal(barrier, inc=1, device_id={"ep": z * side + o}, device_id_type=MESH)
    for j in range(1, n):
        pl.semaphore_signal(barrier, inc=1, device_id=plane(j), device_id_type=MESH)
    pl.semaphore_signal(barrier, inc=1, device_id={"tp": 1 - core}, device_id_type=MESH)

    def send_tok(q, c, to, slot):
        count = k + lax.rem(c, HALF) if slot == 3 else c
        remote(
            tok.at[q, :, cols(c)], tok.at[slot, :, cols(c)],
            s_toks.at[0], s_tok.at[count], plane(to),
        ).start()

    def prep(q):
        ids0, ids1 = met[q, 0:1, :], met[q, 1:2, :]
        wt0, wt1 = met[q, 2:3, :], met[q, 3:4, :]
        row = lax.broadcasted_iota(jnp.int32, (rows, tokens), 0)
        e_row = (z * side + row // cap).astype(jnp.float32)
        s_row = lax.rem(row, cap).astype(jnp.float32)
        hit0 = (ids0 == e_row).astype(jnp.float32)
        hit1 = (ids1 == e_row).astype(jnp.float32)
        hit = hit0 + hit1
        before = (
            lax.broadcasted_iota(jnp.int32, (tokens, tokens), 0)
            < lax.broadcasted_iota(jnp.int32, (tokens, tokens), 1)
        ).astype(jnp.float32).astype(jnp.bfloat16)
        count = jnp.dot(hit.astype(jnp.bfloat16), before, preferred_element_type=jnp.float32)
        pick = jnp.where(count == s_row, hit, 0.0)
        sel[q] = pick.astype(jnp.bfloat16)
        w = pick * (hit0 * wt0 + hit1 * wt1)
        high = w.astype(jnp.bfloat16)
        mix[q, 0] = high
        mix[q, 1] = (w - high.astype(jnp.float32)).astype(jnp.bfloat16)

    @step("prep0")
    def _():
        for copy in firsts[3:]:
            copy.wait()
        met[0, 0:2, :] = ids[...].astype(jnp.float32)
        met[0, 2:4, :] = wts[...]
        met[0, 4:8, :] = jnp.zeros((4, tokens), jnp.float32)
        prep(0)

    @step("raw")
    def _():
        for copy in firsts[:3]:
            copy.wait()

    slab = min(32, tokens)
    lanes = part.shape[1]

    @step("stats")
    def _():
        def total(i, f):
            at = pl.ds(pl.multiple_of(i * slab, slab), slab)
            parts = [
                f(src[at, j * lanes : (j + 1) * lanes].astype(jnp.float32), at)
                for j in range(width // lanes)
            ]
            while len(parts) > 1:
                parts = [a + b for a, b in zip(parts[::2], parts[1::2])]
            part[at, :] = parts[0]

        pl.loop(0, tokens // slab)(lambda i: total(i, lambda v, at: v))
        mu[...] = jnp.sum(part[...], axis=-1, keepdims=True) / width

        def square(v, at):
            v = v - mu[at, :]
            return v * v

        pl.loop(0, tokens // slab)(lambda i: total(i, square))
        rs[...] = lax.rsqrt(jnp.sum(part[...], axis=-1, keepdims=True) / width + 1e-05)

    def fresh(c):
        v = (src[:, cols(c)].astype(jnp.float32) - mu[...]) * rs[...]
        tok[0, :, cols(c)] = (v * gn[:, cols(c)] + bs[:, cols(c)]).astype(jnp.bfloat16)

    def select(q, c):
        v = jnp.dot(sel[q], tok[q, :, cols(c)], preferred_element_type=jnp.float32)
        snd[q, :, cols(c)] = v.astype(jnp.bfloat16)
        xin[q, band(p), cols(c)] = snd[q, band(p), cols(c)]

    def ship(q, c):
        for o in peers:
            remote(
                snd.at[q, band(o), cols(c)], xin.at[q, band(p), cols(c)],
                s_xs.at[0], s_x.at[q], {"ep": z * side + o},
            ).start()

    def disp(q, c):
        select(q, c)
        ship(q, c)

    @step("early")
    def _():
        for c in range(EARLY):
            fresh(c)
            select(0, c)

    @step("meet")
    def _():
        pl.semaphore_wait(barrier, side - 1 + n)

    @step("own")
    def _():
        for to, slot in [(up, 2), (back, 1), (over, 3)]:
            remote(met.at[0], met.at[slot], s_met.at[0], s_met.at[1], plane(to)).start()

    def others(ref, q):
        return ref.at[q, pl.ds(0, (side - 1) * cap)]

    tile = min(256, half)
    per = half // tile

    def gate(q, i):
        h, at = i // per, lax.rem(i, per)
        part = pl.ds(pl.multiple_of(at * tile, tile), tile)
        x = xin[q]
        g = jnp.dot(x, wg[h, :, part], preferred_element_type=jnp.float32)
        u = jnp.dot(x, wu[h, :, part], preferred_element_type=jnp.float32)
        v = g / (1.0 + jnp.exp(-g)) * u
        hid[q, :, pl.ds(pl.multiple_of(i * tile, tile), tile)] = v.astype(jnp.bfloat16)

    def gates(q):
        pl.loop(0, 2 * per)(lambda i: gate(q, i))

    def product(q, c):
        y = jnp.dot(hid[q], wd[:, cols(c)], preferred_element_type=jnp.float32)
        res[q, :, cols(c)] = y.astype(jnp.bfloat16)
        ret[q, band(p), cols(c)] = res[q, band(p), cols(c)]

    def pick(q, c):
        if q == 0:
            return c
        if q == 3:
            return k + lax.rem(c, HALF)
        return k + HALF + lax.rem(c + (HALF if q == 1 else 0), k)

    def give(q, c):
        for o in peers:
            remote(
                res.at[q, band(o), cols(c)], ret.at[q, band(p), cols(c)],
                s_rs.at[0], s_r.at[pick(q, c)], {"ep": z * side + o},
            ).start()

    def down(q, c):
        product(q, c)
        give(q, c)

    def weigh(q, c):
        r = ret[q, :, cols(c)]
        dims = (((0,), (0,)), ((), ()))
        return lax.dot_general(
            mix[q, 0], r, dims, preferred_element_type=jnp.float32
        ) + lax.dot_general(mix[q, 1], r, dims, preferred_element_type=jnp.float32)

    def combine(q, c, to, slot, add):
        v = weigh(q, c)
        if add:
            v = v + racc[2, c].astype(jnp.float32)
        psend[q - 1, c] = v.astype(jnp.bfloat16)
        count = k + lax.rem(c, HALF) if slot == 2 else c
        remote(
            psend.at[q - 1, c], racc.at[slot, c], s_ps.at[0], s_p.at[count], plane(to)
        ).start()

    def back_in(q, c):
        landed(ret.at[q, pl.ds(0, (side - 1) * cap), pl.ds(0, 2 * wide)], s_r.at[pick(q, c)])

    def summed(i):
        landed(racc.at[0, pl.ds(0, 2)], s_p.at[i])

    def arrived(i):
        landed(tok.at[1, :, pl.ds(0, 2 * wide)], s_tok.at[i])

    halfrows = pl.ds(pl.multiple_of(core * half, half), half)
    pairs = [
        (gw.at[0], wg.at[core]), (uw.at[0], wu.at[core]), (dw.at[0], wd.at[halfrows]),
    ]

    def spread(c):
        send_tok(0, c, up, 2)
        send_tok(0, c, back, 1)
        ship(0, c)

    def first(c):
        fresh(c)
        select(0, c)
        spread(c)

    @step("disp0")
    def _():
        pl.loop(0, EARLY)(spread)
        for i, (a, b) in enumerate(pairs):
            pltpu.make_async_copy(a, b, s_w.at[i]).start()
            remote(a, b, s_ws.at[i // 2], s_w.at[i], {"tp": 1 - core}).start()
        pl.loop(EARLY, k)(first)

    @step("preps")
    def _():
        landed(met.at[pl.ds(1, n - 1)], s_met.at[1])
        for q in (1, 2, 3):
            prep(q)

    @step("disp12a")
    def _():
        @pl.loop(0, HALF)
        def _(c):
            arrived(c)
            send_tok(2, c, up, 3)
            disp(1, c)
            disp(2, c)

    @step("disp12b")
    def _():
        @pl.loop(HALF, k)
        def _(c):
            arrived(c)
            send_tok(1, c, back, 3)
            disp(1, c)
            disp(2, c)

    @step("weights")
    def _():
        for i, ref in enumerate((wg, wu, wd)):
            landed(ref, s_w.at[i])

    @step("in0")
    def _():
        landed(others(xin, 0), s_x.at[0])

    turns = 2 * per // HALF if 2 * per >= HALF else 1

    @step("disp3gate0")
    def _():
        @pl.loop(0, HALF)
        def _(i):
            arrived(k + i)
            for c in (i, i + HALF):
                disp(3, c)
            for j in range(turns):
                gate(0, i * turns + j)

    @step("product0")
    def _():
        pl.loop(0, k)(lambda c: product(0, c))

    @step("in1")
    def _():
        landed(others(xin, 1), s_x.at[1])

    @step("gates1")
    def _():
        gates(1)

    @step("down1")
    def _():
        pl.loop(HALF, k)(lambda c: down(1, c))

    @step("in2")
    def _():
        landed(others(xin, 2), s_x.at[2])

    @step("gates2")
    def _():
        gates(2)

    @step("down2")
    def _():
        pl.loop(0, HALF)(lambda c: down(2, c))

    @step("in3")
    def _():
        landed(others(xin, 3), s_x.at[3])

    @step("gates3")
    def _():
        gates(3)

    @step("down3")
    def _():
        @pl.loop(0, HALF)
        def _(i):
            down(3, i)
            down(3, i + HALF)
            back_in(2, i)
            combine(1, i + HALF, up, 0, False)
            combine(2, i, back, 1, False)

    @step("down12")
    def _():
        @pl.loop(0, HALF)
        def _(i):
            down(1, i)
            down(2, i + HALF)

    @step("give0")
    def _():
        pl.loop(0, k)(lambda c: give(0, c))

    @step("comb3")
    def _():
        @pl.loop(0, HALF)
        def _(i):
            back_in(3, i)
            combine(3, i, up, 2, False)
            combine(3, i + HALF, back, 2, False)

    @step("comb12b")
    def _():
        @pl.loop(0, HALF)
        def _(i):
            back_in(1, i)
            summed(k + i)
            combine(1, i, up, 0, True)
            combine(2, i + HALF, back, 1, True)

    @step("drain")
    def _():
        landed(met.at[pl.ds(1, n - 1)], s_met.at[0])
        landed(wg, s_ws.at[0])
        landed(wd.at[halfrows], s_ws.at[1])
        landed(tok.at[pl.ds(0, n - 1)], s_toks.at[0])
        landed(snd.at[:, pl.ds(0, (side - 1) * cap)], s_xs.at[0])

    @step("last")
    def _():
        @pl.loop(0, k)
        def _(c):
            with jax.named_scope("wr"):
                landed(ret.at[0, pl.ds(0, (side - 1) * cap), cols(c)], s_r.at[pick(0, c)])
            with jax.named_scope("wp"):
                summed(c)
            y = weigh(0, c)
            for slot in (0, 1):
                y = y + racc[slot, c].astype(jnp.float32)
            out[:, cols(c)] = y.astype(out.dtype)

    @step("end")
    def _():
        landed(psend, s_ps.at[0])
        landed(res.at[:, pl.ds(0, (side - 1) * cap)], s_rs.at[0])


def body(
    tokens, norm_gain, norm_bias, gate_weight, up_weight, down_weight, expert_ids, route_weights
):
    count, width = tokens.shape
    experts = lax.axis_size("ep")
    cap = max(4 * count // experts, 4)
    side = experts // LINE
    half = gate_weight.shape[2]
    rows = side * cap
    wide = width // CHUNKS
    bf = jnp.bfloat16
    dma = pltpu.SemaphoreType.DMA
    hbm = pl.BlockSpec(memory_space=pl.ANY)
    return pl.pallas_call(
        functools.partial(kernel, side),
        out_shape=pltpu.VMEM((count, width), bf),
        in_specs=[hbm] * 8,
        out_specs=pl.BlockSpec(memory_space=pltpu.VMEM),
        scratch_shapes=[
            pltpu.VMEM((count, width), bf),
            pltpu.VMEM((1, width), jnp.float32),
            pltpu.VMEM((1, width), jnp.float32),
            pltpu.VMEM((count, 128), jnp.float32),
            pltpu.VMEM((count, 1), jnp.float32),
            pltpu.VMEM((count, 1), jnp.float32),
            pltpu.VMEM((2, count), jnp.int32),
            pltpu.VMEM((2, count), jnp.float32),
            pltpu.VMEM((LINE, count, width), bf),
            pltpu.VMEM((LINE, 8, count), jnp.float32),
            pltpu.VMEM((2, width, half), bf),
            pltpu.VMEM((2, width, half), bf),
            pltpu.VMEM((2 * half, width), bf),
            pltpu.VMEM((LINE, rows, count), bf),
            pltpu.VMEM((LINE, 2, rows, count), bf),
            pltpu.VMEM((LINE, rows, width), bf),
            pltpu.VMEM((LINE, rows, width), bf),
            pltpu.VMEM((LINE, rows, 2 * half), bf),
            pltpu.VMEM((LINE, rows, width), bf),
            pltpu.VMEM((LINE, rows, width), bf),
            pltpu.VMEM((LINE - 1, CHUNKS, count, wide), bf),
            pltpu.VMEM((LINE - 1, CHUNKS, count, wide), bf),
            dma((5,)),
            dma((2,)),
            dma((3,)),
            dma((2,)),
            dma((CHUNKS + HALF,)),
            dma((1,)),
            dma((LINE,)),
            dma((1,)),
            dma((2 * CHUNKS + HALF,)),
            dma((1,)),
            dma((CHUNKS + HALF,)),
            dma((1,)),
        ],
        compiler_params=pltpu.CompilerParams(
            collective_id=0, has_side_effects=True, vmem_limit_bytes=52 * 1024 * 1024
        ),
    )(
        *[
            pltpu.with_memory_space_constraint(a, pltpu.HBM)
            for a in (
                tokens, norm_gain[None], norm_bias[None], expert_ids.T, route_weights.T,
                gate_weight, up_weight, down_weight,
            )
        ]
    )


def solution(mesh):
    placed = (
        P(("ep", "tp"), None),
        P(),
        P(),
        P("ep", None, "tp"),
        P("ep", None, "tp"),
        P("ep", "tp", None),
        P(("ep", "tp"), None),
        P(("ep", "tp"), None),
    )
    return jax.shard_map(
        body, mesh=mesh, in_specs=placed, out_specs=P(("ep", "tp"), None), check_vma=False
    )
```

```python
import functools

import jax
import jax.numpy as jnp
from jax import lax
from jax.experimental import pallas as pl
from jax.experimental.pallas import tpu as pltpu
from jax.sharding import PartitionSpec as P

MESH = pl.DeviceIdType.MESH
LINE = 4
CHUNKS = 8
HALF = CHUNKS // 2
EARLY = 2
X, Y, Z = 0, 1, 2
SIDEWAYS = [(0, X), (1, Y)]
SPLIT = len(SIDEWAYS)
MIDDLE = (SPLIT + CHUNKS) // 2


def kernel(
    planes, raw, gain, bias, idsin, wtin, gw, uw, dw, out,
    src, gn, bs, part, mu, rs, ids, wts, tok, met, wg, wu, wd, sel, mix, snd, xin, hid, res, ret, psend, racc,
    s_own, s_met, s_w, s_ws, s_tok, s_toks, s_x, s_xs, s_r, s_rs, s_p, s_ps,
):
    n = LINE
    side = planes
    me, core = lax.axis_index("ep"), lax.axis_index("tp")
    z, p = me // side, lax.rem(me, side)
    y, x = p // LINE, lax.rem(p, LINE)
    tokens, width = raw.shape
    half = gw.shape[2]
    rows = snd.shape[1]
    cap = rows // side
    k = CHUNKS
    wide = width // k

    def cols(c):
        return pl.ds(pl.multiple_of(c * wide, wide), wide)

    def band(i):
        return pl.ds(pl.multiple_of(i * cap, cap), cap)

    def plane(j):
        return {"ep": lax.rem(z + j, n) * side + p}

    up, over, back = 1, 2, n - 1
    role = {0: 0, up: 1, back: 2, over: 3}
    steps = {q: j for j, q in role.items()}

    def ident(a, b, c):
        return {"ep": a * side + b * n + c}

    def turn(a, j):
        return lax.rem(a + j, n) if j else a

    def ring(way, j):
        return ident(
            turn(z, j if way == Z else 0), turn(y, j if way == Y else 0), turn(x, j if way == X else 0)
        )


    def away(d):
        return sum(min(j, n - j) for j in d)

    offsets = [(b, c) for b in range(n) for c in range(n) if b or c]
    peers = [
        lax.rem(y + b, n) * n + lax.rem(x + c, n)
        for b, c in sorted(offsets, key=lambda d: -away(d))
    ]

    def remote(src, dst, send, recv, where):
        return pltpu.make_async_remote_copy(
            src_ref=src, dst_ref=dst, send_sem=send, recv_sem=recv,
            device_id=where, device_id_type=MESH,
        )

    def landed(ref, sem):
        pltpu.make_async_copy(ref, ref, sem).wait()

    def step(name):
        def run(f):
            with jax.named_scope(name):
                f()
        return run

    firsts = [
        pltpu.make_async_copy(a, b, s_own.at[i])
        for i, (a, b) in enumerate(
            [(raw, src), (gain, gn), (bias, bs), (idsin, ids), (wtin, wts)]
        )
    ]
    for copy in firsts:
        copy.start()
    barrier = pltpu.get_barrier_semaphore()
    for o in peers:
        pl.semaphore_signal(barrier, inc=1, device_id={"ep": z * side + o}, device_id_type=MESH)
    for j in range(1, n):
        pl.semaphore_signal(barrier, inc=1, device_id=plane(j), device_id_type=MESH)
    pl.semaphore_signal(barrier, inc=1, device_id={"tp": 1 - core}, device_id_type=MESH)

    def send_tok(way, q, c, to, slot, part=None):
        if slot < 3:
            count = c
        elif way == Z:
            count = k + SPLIT + lax.rem(c - SPLIT, MIDDLE - SPLIT)
        else:
            count = k + c
        at = cols(c)
        if part is not None:
            at = pl.ds(c * wide + part * (wide // 2), wide // 2)
        remote(
            tok.at[q, :, at], tok.at[slot, :, at], s_toks.at[0], s_tok.at[count], ring(way, to)
        ).start()

    def prep(way, q):
        at = (way, q) if q else (Z, 0)
        ids0, ids1 = met[at + (slice(0, 1),)], met[at + (slice(1, 2),)]
        wt0, wt1 = met[at + (slice(2, 3),)], met[at + (slice(3, 4),)]
        row = lax.broadcasted_iota(jnp.int32, (rows, tokens), 0)
        which = row // cap
        far, close = which // n, lax.rem(which, n)
        expert = [
            far * side + close * n + x, far * side + y * n + close, z * side + which
        ][way]
        e_row = expert.astype(jnp.float32)
        s_row = lax.rem(row, cap).astype(jnp.float32)
        hit0 = (ids0 == e_row).astype(jnp.float32)
        hit1 = (ids1 == e_row).astype(jnp.float32)
        hit = hit0 + hit1
        before = (
            lax.broadcasted_iota(jnp.int32, (tokens, tokens), 0)
            < lax.broadcasted_iota(jnp.int32, (tokens, tokens), 1)
        ).astype(jnp.float32).astype(jnp.bfloat16)
        count = jnp.dot(hit.astype(jnp.bfloat16), before, preferred_element_type=jnp.float32)
        pick = jnp.where(count == s_row, hit, 0.0)
        sel[way, q] = pick.astype(jnp.bfloat16)
        if way == Z:
            w = pick * (hit0 * wt0 + hit1 * wt1)
            high = w.astype(jnp.bfloat16)
            mix[q, 0] = high
            mix[q, 1] = (w - high.astype(jnp.float32)).astype(jnp.bfloat16)

    @step("prep0")
    def _():
        for copy in firsts[3:]:
            copy.wait()
        met[Z, 0, 0:2, :] = ids[...].astype(jnp.float32)
        met[Z, 0, 2:4, :] = wts[...]
        met[Z, 0, 4:8, :] = jnp.zeros((4, tokens), jnp.float32)
        prep(Z, 0)

    @step("raw")
    def _():
        for copy in firsts[:3]:
            copy.wait()

    slab = min(32, tokens)
    lanes = part.shape[1]

    @step("stats")
    def _():
        def total(i, f):
            at = pl.ds(pl.multiple_of(i * slab, slab), slab)
            parts = [
                f(src[at, j * lanes : (j + 1) * lanes].astype(jnp.float32), at)
                for j in range(width // lanes)
            ]
            while len(parts) > 1:
                parts = [a + b for a, b in zip(parts[::2], parts[1::2])]
            part[at, :] = parts[0]

        pl.loop(0, tokens // slab)(lambda i: total(i, lambda v, at: v))
        mu[...] = jnp.sum(part[...], axis=-1, keepdims=True) / width

        def square(v, at):
            v = v - mu[at, :]
            return v * v

        pl.loop(0, tokens // slab)(lambda i: total(i, square))
        rs[...] = lax.rsqrt(jnp.sum(part[...], axis=-1, keepdims=True) / width + 1e-05)

    def fresh(c):
        v = (src[:, cols(c)].astype(jnp.float32) - mu[...]) * rs[...]
        tok[0, :, cols(c)] = (v * gn[:, cols(c)] + bs[:, cols(c)]).astype(jnp.bfloat16)

    def select(way, q, c):
        v = jnp.dot(sel[way, q], tok[q, :, cols(c)], preferred_element_type=jnp.float32)
        snd[q, :, cols(c)] = v.astype(jnp.bfloat16)

    def ship(way, q, c):
        if way == Z:
            xin[q, band(p), cols(c)] = snd[q, band(p), cols(c)]
            for o in peers:
                remote(
                    snd.at[q, band(o), cols(c)], xin.at[q, band(p), cols(c)],
                    s_xs.at[0], s_x.at[1, q], {"ep": z * side + o},
                ).start()
            return
        j = steps[q]
        for a, b in [(0, 0)] + sorted(offsets, key=lambda d: -away(d)):
            far = turn(z, a)
            if way == X:
                close = turn(y, b)
                where, to = ident(far, close, x), y * n + turn(x, j)
            else:
                close = turn(x, b)
                where, to = ident(far, y, close), turn(y, j) * n + x
            got = xin.at[role[(n - a) % n], band(to), cols(c)]
            row = band(far * n + close)
            if a or b:
                remote(
                    snd.at[q, row, cols(c)], got, s_xs.at[0], s_x.at[0, role[(n - a) % n]], where
                ).start()
            else:
                xin[0, band(to), cols(c)] = snd[q, row, cols(c)]

    def disp(way, q, c):
        select(way, q, c)
        ship(way, q, c)

    def ready(q):
        count = (side - n if q == 0 else side) * cap
        landed(xin.at[q, pl.ds(0, count), pl.ds(0, SPLIT * wide)], s_x.at[0, q])
        landed(xin.at[q, pl.ds(0, (side - 1) * cap), pl.ds(SPLIT * wide, (k - SPLIT) * wide)], s_x.at[1, q])

    @step("early")
    def _():
        for c, _ in SIDEWAYS:
            fresh(c)
        for c in range(SPLIT, SPLIT + EARLY):
            fresh(c)
            select(Z, 0, c)

    @step("meet")
    def _():
        pl.semaphore_wait(barrier, side - 1 + n)

    @step("own")
    def _():
        for way in (Z, X, Y):
            for q in range(1, n):
                slot = role[n - steps[q]]
                remote(
                    met.at[Z, 0], met.at[way, slot], s_met.at[3], s_met.at[way], ring(way, steps[q])
                ).start()

    def others(ref, q):
        return ref.at[q, pl.ds(0, (side - 1) * cap)]

    tile = min(256, half)
    per = half // tile

    def gate(q, i):
        h, at = i // per, lax.rem(i, per)
        part = pl.ds(pl.multiple_of(at * tile, tile), tile)
        x = xin[q]
        g = jnp.dot(x, wg[h, :, part], preferred_element_type=jnp.float32)
        u = jnp.dot(x, wu[h, :, part], preferred_element_type=jnp.float32)
        v = g / (1.0 + jnp.exp(-g)) * u
        hid[q, :, pl.ds(pl.multiple_of(i * tile, tile), tile)] = v.astype(jnp.bfloat16)

    def gates(q):
        pl.loop(0, 2 * per)(lambda i: gate(q, i))

    def product(q, c):
        y = jnp.dot(hid[q], wd[:, cols(c)], preferred_element_type=jnp.float32)
        res[q, :, cols(c)] = y.astype(jnp.bfloat16)
        ret[q, band(p), cols(c)] = res[q, band(p), cols(c)]

    def pick(q, c):
        if q == 0:
            return c
        if q == 3:
            return k + lax.rem(c, HALF)
        return k + HALF + lax.rem(c + (HALF if q == 1 else 0), k)

    def give(q, c):
        for o in peers:
            remote(
                res.at[q, band(o), cols(c)], ret.at[q, band(p), cols(c)],
                s_rs.at[0], s_r.at[pick(q, c)], {"ep": z * side + o},
            ).start()

    def down(q, c):
        product(q, c)
        give(q, c)

    def weigh(q, c):
        r = ret[q, :, cols(c)]
        dims = (((0,), (0,)), ((), ()))
        return lax.dot_general(
            mix[q, 0], r, dims, preferred_element_type=jnp.float32
        ) + lax.dot_general(mix[q, 1], r, dims, preferred_element_type=jnp.float32)

    def combine(q, c, to, slot, add):
        v = weigh(q, c)
        if add:
            v = v + racc[2, c].astype(jnp.float32)
        psend[q - 1, c] = v.astype(jnp.bfloat16)
        count = k + lax.rem(c, HALF) if slot == 2 else c
        remote(
            psend.at[q - 1, c], racc.at[slot, c], s_ps.at[0], s_p.at[count], plane(to)
        ).start()

    def back_in(q, c):
        landed(ret.at[q, pl.ds(0, (side - 1) * cap), pl.ds(0, 2 * wide)], s_r.at[pick(q, c)])

    def summed(i):
        landed(racc.at[0, pl.ds(0, 2)], s_p.at[i])

    def arrived(i):
        landed(tok.at[1, :, pl.ds(0, 2 * wide)], s_tok.at[i])

    halfrows = pl.ds(pl.multiple_of(core * half, half), half)
    pairs = [
        (gw.at[0], wg.at[core]), (uw.at[0], wu.at[core]), (dw.at[0], wd.at[halfrows]),
    ]

    def around(way, c):
        send_tok(way, 0, c, up, 2)
        send_tok(way, 0, c, back, 1)

    def spread(c):
        around(Z, c)
        ship(Z, 0, c)

    def first(c):
        fresh(c)
        select(Z, 0, c)
        spread(c)

    @step("disp0")
    def _():
        for c, way in SIDEWAYS:
            around(way, c)
        pl.loop(SPLIT, SPLIT + EARLY)(spread)
        for i, (a, b) in enumerate(pairs):
            pltpu.make_async_copy(a, b, s_w.at[i]).start()
            remote(a, b, s_ws.at[i // 2], s_w.at[i], {"tp": 1 - core}).start()
        pl.loop(SPLIT + EARLY, k)(first)

    @step("preps")
    def _():
        for way in (Z, X, Y):
            landed(met.at[way, pl.ds(1, n - 1)], s_met.at[way])
            for q in range(0 if way != Z else 1, n):
                prep(way, q)

    @step("besxy")
    def _():
        for c, way in SIDEWAYS:
            arrived(c)
            send_tok(way, 2, c, up, 3, 0)
            send_tok(way, 1, c, back, 3, 1)
        for c, way in SIDEWAYS:
            for q in range(3):
                disp(way, q, c)

    @step("besza")
    def _():
        @pl.loop(SPLIT, MIDDLE)
        def _(c):
            arrived(c)
            send_tok(Z, 2, c, up, 3)
            disp(Z, 1, c)
            disp(Z, 2, c)

    @step("acrxy")
    def _():
        for c, way in SIDEWAYS:
            landed(tok.at[3, :, cols(c)], s_tok.at[k + c])
            disp(way, 3, c)

    @step("beszb")
    def _():
        @pl.loop(MIDDLE, k)
        def _(c):
            arrived(c)
            send_tok(Z, 1, c, back, 3)
            disp(Z, 1, c)
            disp(Z, 2, c)

    @step("acrz")
    def _():
        @pl.loop(0, MIDDLE - SPLIT)
        def _(i):
            arrived(k + SPLIT + i)
            disp(Z, 3, SPLIT + i)
            disp(Z, 3, MIDDLE + i)

    @step("weights")
    def _():
        for i, ref in enumerate((wg, wu, wd)):
            landed(ref, s_w.at[i])

    @step("in1")
    def _():
        ready(1)

    @step("gates1")
    def _():
        gates(1)

    @step("down1")
    def _():
        pl.loop(HALF, k)(lambda c: down(1, c))

    @step("in2")
    def _():
        ready(2)

    @step("gates2")
    def _():
        gates(2)

    @step("down2")
    def _():
        pl.loop(0, HALF)(lambda c: down(2, c))

    @step("in3")
    def _():
        ready(3)

    @step("gates3")
    def _():
        gates(3)

    @step("down3")
    def _():
        @pl.loop(0, HALF)
        def _(i):
            down(3, i)
            down(3, i + HALF)
            back_in(2, i)
            combine(1, i + HALF, up, 0, False)
            combine(2, i, back, 1, False)

    @step("down12c3")
    def _():
        @pl.loop(0, HALF)
        def _(i):
            down(1, i)
            down(2, i + HALF)
            back_in(3, i)
            combine(3, i, up, 2, False)
            combine(3, i + HALF, back, 2, False)

    @step("gates0")
    def _():
        ready(0)
        gates(0)

    @step("down0")
    def _():
        pl.loop(0, k)(lambda c: down(0, c))

    @step("comb12b")
    def _():
        @pl.loop(0, HALF)
        def _(i):
            back_in(1, i)
            summed(k + i)
            combine(1, i, up, 0, True)
            combine(2, i + HALF, back, 1, True)

    @step("drain")
    def _():
        landed(met.at[:, pl.ds(1, n - 1)], s_met.at[3])
        landed(wg, s_ws.at[0])
        landed(wd.at[halfrows], s_ws.at[1])
        landed(tok.at[pl.ds(0, n - 1)], s_toks.at[0])
        landed(snd.at[:, pl.ds(0, (side - 1) * cap)], s_xs.at[0])

    @step("last")
    def _():
        @pl.loop(0, k)
        def _(c):
            with jax.named_scope("wr"):
                landed(ret.at[0, pl.ds(0, (side - 1) * cap), cols(c)], s_r.at[pick(0, c)])
            with jax.named_scope("wp"):
                summed(c)
            y = weigh(0, c)
            for slot in (0, 1):
                y = y + racc[slot, c].astype(jnp.float32)
            out[:, cols(c)] = y.astype(out.dtype)

    @step("end")
    def _():
        landed(psend, s_ps.at[0])
        landed(res.at[:, pl.ds(0, (side - 1) * cap)], s_rs.at[0])


def body(
    tokens, norm_gain, norm_bias, gate_weight, up_weight, down_weight, expert_ids, route_weights
):
    count, width = tokens.shape
    experts = lax.axis_size("ep")
    cap = max(4 * count // experts, 4)
    side = experts // LINE
    half = gate_weight.shape[2]
    rows = side * cap
    wide = width // CHUNKS
    bf = jnp.bfloat16
    dma = pltpu.SemaphoreType.DMA
    hbm = pl.BlockSpec(memory_space=pl.ANY)
    return pl.pallas_call(
        functools.partial(kernel, side),
        out_shape=pltpu.VMEM((count, width), bf),
        in_specs=[hbm] * 8,
        out_specs=pl.BlockSpec(memory_space=pltpu.VMEM),
        scratch_shapes=[
            pltpu.VMEM((count, width), bf),
            pltpu.VMEM((1, width), jnp.float32),
            pltpu.VMEM((1, width), jnp.float32),
            pltpu.VMEM((count, 128), jnp.float32),
            pltpu.VMEM((count, 1), jnp.float32),
            pltpu.VMEM((count, 1), jnp.float32),
            pltpu.VMEM((2, count), jnp.int32),
            pltpu.VMEM((2, count), jnp.float32),
            pltpu.VMEM((LINE, count, width), bf),
            pltpu.VMEM((3, LINE, 8, count), jnp.float32),
            pltpu.VMEM((2, width, half), bf),
            pltpu.VMEM((2, width, half), bf),
            pltpu.VMEM((2 * half, width), bf),
            pltpu.VMEM((3, LINE, rows, count), bf),
            pltpu.VMEM((LINE, 2, rows, count), bf),
            pltpu.VMEM((LINE, rows, width), bf),
            pltpu.VMEM((LINE, rows, width), bf),
            pltpu.VMEM((LINE, rows, 2 * half), bf),
            pltpu.VMEM((LINE, rows, width), bf),
            pltpu.VMEM((LINE, rows, width), bf),
            pltpu.VMEM((LINE - 1, CHUNKS, count, wide), bf),
            pltpu.VMEM((LINE - 1, CHUNKS, count, wide), bf),
            dma((5,)),
            dma((4,)),
            dma((3,)),
            dma((2,)),
            dma((CHUNKS + MIDDLE,)),
            dma((1,)),
            dma((2, LINE)),
            dma((1,)),
            dma((2 * CHUNKS + HALF,)),
            dma((1,)),
            dma((CHUNKS + HALF,)),
            dma((1,)),
        ],
        compiler_params=pltpu.CompilerParams(
            collective_id=0, has_side_effects=True, vmem_limit_bytes=52 * 1024 * 1024
        ),
    )(
        *[
            pltpu.with_memory_space_constraint(a, pltpu.HBM)
            for a in (
                tokens, norm_gain[None], norm_bias[None], expert_ids.T, route_weights.T,
                gate_weight, up_weight, down_weight,
            )
        ]
    )


def solution(mesh):
    placed = (
        P(("ep", "tp"), None),
        P(),
        P(),
        P("ep", None, "tp"),
        P("ep", None, "tp"),
        P("ep", "tp", None),
        P(("ep", "tp"), None),
        P(("ep", "tp"), None),
    )
    return jax.shard_map(
        body, mesh=mesh, in_specs=placed, out_specs=P(("ep", "tp"), None), check_vma=False
    )
```

```python
import functools

import jax
import jax.numpy as jnp
from jax import lax
from jax.experimental import pallas as pl
from jax.experimental.pallas import tpu as pltpu
from jax.sharding import PartitionSpec as P

MESH = pl.DeviceIdType.MESH
LINE = 4
CHUNKS = 8
HALF = CHUNKS // 2
EARLY = 1
X, Y, Z = 0, 1, 2
SIDEWAYS = [(0, X), (1, Y)]
SPLIT = len(SIDEWAYS)
MIDDLE = (SPLIT + CHUNKS) // 2


def kernel(
    planes, raw, gain, bias, idsin, wtin, gw, uw, dw, out,
    src, gn, bs, part, mu, rs, ids, wts, tok, met, wg, wu, wd, sel, mix, snd, xin, hid, res, ret, psend, racc,
    s_own, s_met, s_w, s_ws, s_tok, s_toks, s_x, s_xs, s_r, s_rs, s_p, s_ps,
):
    n = LINE
    side = planes
    me, core = lax.axis_index("ep"), lax.axis_index("tp")
    z, p = me // side, lax.rem(me, side)
    y, x = p // LINE, lax.rem(p, LINE)
    tokens, width = raw.shape
    half = gw.shape[2]
    rows = snd.shape[1]
    cap = rows // side
    k = CHUNKS
    wide = width // k

    def cols(c):
        return pl.ds(pl.multiple_of(c * wide, wide), wide)

    def band(i):
        return pl.ds(pl.multiple_of(i * cap, cap), cap)

    def plane(j):
        return {"ep": lax.rem(z + j, n) * side + p}

    up, over, back = 1, 2, n - 1
    role = {0: 0, up: 1, back: 2, over: 3}
    steps = {q: j for j, q in role.items()}

    def ident(a, b, c):
        return {"ep": a * side + b * n + c}

    def turn(a, j):
        return lax.rem(a + j, n) if j else a

    def ring(way, j):
        return ident(
            turn(z, j if way == Z else 0), turn(y, j if way == Y else 0), turn(x, j if way == X else 0)
        )


    def away(d):
        return sum(min(j, n - j) for j in d)

    offsets = [(b, c) for b in range(n) for c in range(n) if b or c]
    peers = [
        lax.rem(y + b, n) * n + lax.rem(x + c, n)
        for b, c in sorted(offsets, key=lambda d: -away(d))
    ]

    def remote(src, dst, send, recv, where):
        return pltpu.make_async_remote_copy(
            src_ref=src, dst_ref=dst, send_sem=send, recv_sem=recv,
            device_id=where, device_id_type=MESH,
        )

    def landed(ref, sem):
        pltpu.make_async_copy(ref, ref, sem).wait()

    def step(name):
        def run(f):
            with jax.named_scope(name):
                f()
        return run

    firsts = [
        pltpu.make_async_copy(a, b, s_own.at[i])
        for i, (a, b) in enumerate(
            [(raw, src), (gain, gn), (bias, bs), (idsin, ids), (wtin, wts)]
        )
    ]
    for copy in firsts:
        copy.start()
    barrier = pltpu.get_barrier_semaphore()
    for o in peers:
        pl.semaphore_signal(barrier, inc=1, device_id={"ep": z * side + o}, device_id_type=MESH)
    for j in range(1, n):
        pl.semaphore_signal(barrier, inc=1, device_id=plane(j), device_id_type=MESH)
    pl.semaphore_signal(barrier, inc=1, device_id={"tp": 1 - core}, device_id_type=MESH)

    def send_tok(way, q, c, to, slot, part=None):
        if slot < 3:
            count = c
        elif way == Z:
            count = k + SPLIT + lax.rem(c - SPLIT, MIDDLE - SPLIT)
        else:
            count = k + c
        at = cols(c)
        if part is not None:
            at = pl.ds(c * wide + part * (wide // 2), wide // 2)
        remote(
            tok.at[q, :, at], tok.at[slot, :, at], s_toks.at[0], s_tok.at[count], ring(way, to)
        ).start()

    def prep(way, q):
        at = (way, q) if q else (Z, 0)
        ids0, ids1 = met[at + (slice(0, 1),)], met[at + (slice(1, 2),)]
        wt0, wt1 = met[at + (slice(2, 3),)], met[at + (slice(3, 4),)]
        row = lax.broadcasted_iota(jnp.int32, (rows, tokens), 0)
        which = row // cap
        far, close = which // n, lax.rem(which, n)
        expert = [
            far * side + close * n + x, far * side + y * n + close, z * side + which
        ][way]
        e_row = expert.astype(jnp.float32)
        s_row = lax.rem(row, cap).astype(jnp.float32)
        hit0 = (ids0 == e_row).astype(jnp.float32)
        hit1 = (ids1 == e_row).astype(jnp.float32)
        hit = hit0 + hit1
        before = (
            lax.broadcasted_iota(jnp.int32, (tokens, tokens), 0)
            < lax.broadcasted_iota(jnp.int32, (tokens, tokens), 1)
        ).astype(jnp.float32).astype(jnp.bfloat16)
        count = jnp.dot(hit.astype(jnp.bfloat16), before, preferred_element_type=jnp.float32)
        pick = jnp.where(count == s_row, hit, 0.0)
        sel[way, q] = pick.astype(jnp.bfloat16)
        if way == Z:
            w = pick * (hit0 * wt0 + hit1 * wt1)
            high = w.astype(jnp.bfloat16)
            mix[q, 0] = high
            mix[q, 1] = (w - high.astype(jnp.float32)).astype(jnp.bfloat16)

    @step("prep0")
    def _():
        for copy in firsts[3:]:
            copy.wait()
        met[Z, 0, 0:2, :] = ids[...].astype(jnp.float32)
        met[Z, 0, 2:4, :] = wts[...]
        met[Z, 0, 4:8, :] = jnp.zeros((4, tokens), jnp.float32)
        prep(Z, 0)

    @step("raw")
    def _():
        for copy in firsts[:3]:
            copy.wait()

    slab = min(32, tokens)
    lanes = part.shape[1]

    @step("stats")
    def _():
        def total(i, f):
            at = pl.ds(pl.multiple_of(i * slab, slab), slab)
            parts = [
                f(src[at, j * lanes : (j + 1) * lanes].astype(jnp.float32), at)
                for j in range(width // lanes)
            ]
            while len(parts) > 1:
                parts = [a + b for a, b in zip(parts[::2], parts[1::2])]
            part[at, :] = parts[0]

        pl.loop(0, tokens // slab)(lambda i: total(i, lambda v, at: v))
        mu[...] = jnp.sum(part[...], axis=-1, keepdims=True) / width

        def square(v, at):
            v = v - mu[at, :]
            return v * v

        pl.loop(0, tokens // slab)(lambda i: total(i, square))
        rs[...] = lax.rsqrt(jnp.sum(part[...], axis=-1, keepdims=True) / width + 1e-05)

    def fresh(c):
        v = (src[:, cols(c)].astype(jnp.float32) - mu[...]) * rs[...]
        tok[0, :, cols(c)] = (v * gn[:, cols(c)] + bs[:, cols(c)]).astype(jnp.bfloat16)

    def select(way, q, c):
        v = jnp.dot(sel[way, q], tok[q, :, cols(c)], preferred_element_type=jnp.float32)
        snd[q, :, cols(c)] = v.astype(jnp.bfloat16)

    def ship(way, q, c):
        if way == Z:
            xin[q, band(p), cols(c)] = snd[q, band(p), cols(c)]
            for o in peers:
                remote(
                    snd.at[q, band(o), cols(c)], xin.at[q, band(p), cols(c)],
                    s_xs.at[0], s_x.at[1, q], {"ep": z * side + o},
                ).start()
            return
        j = steps[q]
        for a, b in [(0, 0)] + sorted(offsets, key=lambda d: -away(d)):
            far = turn(z, a)
            if way == X:
                close = turn(y, b)
                where, to = ident(far, close, x), y * n + turn(x, j)
            else:
                close = turn(x, b)
                where, to = ident(far, y, close), turn(y, j) * n + x
            got = xin.at[role[(n - a) % n], band(to), cols(c)]
            row = band(far * n + close)
            if a or b:
                remote(
                    snd.at[q, row, cols(c)], got, s_xs.at[0], s_x.at[0, role[(n - a) % n]], where
                ).start()
            else:
                xin[0, band(to), cols(c)] = snd[q, row, cols(c)]

    def disp(way, q, c):
        select(way, q, c)
        ship(way, q, c)

    def ready(q):
        count = (side - n if q == 0 else side) * cap
        landed(xin.at[q, pl.ds(0, count), pl.ds(0, SPLIT * wide)], s_x.at[0, q])
        landed(xin.at[q, pl.ds(0, (side - 1) * cap), pl.ds(SPLIT * wide, (k - SPLIT) * wide)], s_x.at[1, q])

    @step("early")
    def _():
        for c in range(SPLIT, SPLIT + EARLY):
            fresh(c)
            select(Z, 0, c)

    @step("meet")
    def _():
        pl.semaphore_wait(barrier, side - 1 + n)

    @step("own")
    def _():
        for way in (Z, X, Y):
            for q in range(1, n):
                slot = role[n - steps[q]]
                remote(
                    met.at[Z, 0], met.at[way, slot], s_met.at[3], s_met.at[way], ring(way, steps[q])
                ).start()

    def others(ref, q):
        return ref.at[q, pl.ds(0, (side - 1) * cap)]

    tile = min(256, half)
    per = half // tile

    def gate(q, i):
        h, at = i // per, lax.rem(i, per)
        part = pl.ds(pl.multiple_of(at * tile, tile), tile)
        x = xin[q]
        g = jnp.dot(x, wg[h, :, part], preferred_element_type=jnp.float32)
        u = jnp.dot(x, wu[h, :, part], preferred_element_type=jnp.float32)
        v = g / (1.0 + jnp.exp(-g)) * u
        hid[q, :, pl.ds(pl.multiple_of(i * tile, tile), tile)] = v.astype(jnp.bfloat16)

    def gates(q):
        pl.loop(0, 2 * per)(lambda i: gate(q, i))

    def product(q, c):
        y = jnp.dot(hid[q], wd[:, cols(c)], preferred_element_type=jnp.float32)
        res[q, :, cols(c)] = y.astype(jnp.bfloat16)
        ret[q, band(p), cols(c)] = res[q, band(p), cols(c)]

    def pick(q, c):
        if q == 0:
            return c
        if q == 3:
            return k + lax.rem(c, HALF)
        return k + HALF + lax.rem(c + (HALF if q == 1 else 0), k)

    def give(q, c):
        for o in peers:
            remote(
                res.at[q, band(o), cols(c)], ret.at[q, band(p), cols(c)],
                s_rs.at[0], s_r.at[pick(q, c)], {"ep": z * side + o},
            ).start()

    def down(q, c):
        product(q, c)
        give(q, c)

    def weigh(q, c):
        r = ret[q, :, cols(c)]
        dims = (((0,), (0,)), ((), ()))
        return lax.dot_general(
            mix[q, 0], r, dims, preferred_element_type=jnp.float32
        ) + lax.dot_general(mix[q, 1], r, dims, preferred_element_type=jnp.float32)

    def combine(q, c, to, slot, add):
        v = weigh(q, c)
        if add:
            v = v + racc[2, c].astype(jnp.float32)
        psend[q - 1, c] = v.astype(jnp.bfloat16)
        count = k + lax.rem(c, HALF) if slot == 2 else c
        remote(
            psend.at[q - 1, c], racc.at[slot, c], s_ps.at[0], s_p.at[count], plane(to)
        ).start()

    def back_in(q, c):
        landed(ret.at[q, pl.ds(0, (side - 1) * cap), pl.ds(0, 2 * wide)], s_r.at[pick(q, c)])

    def summed(i):
        landed(racc.at[0, pl.ds(0, 2)], s_p.at[i])

    def arrived(i):
        landed(tok.at[1, :, pl.ds(0, 2 * wide)], s_tok.at[i])

    halfrows = pl.ds(pl.multiple_of(core * half, half), half)
    pairs = [
        (gw.at[0], wg.at[core]), (uw.at[0], wu.at[core]), (dw.at[0], wd.at[halfrows]),
    ]

    def around(way, c):
        send_tok(way, 0, c, up, 2)
        send_tok(way, 0, c, back, 1)

    def spread(c):
        around(Z, c)
        ship(Z, 0, c)

    def first(c):
        fresh(c)
        select(Z, 0, c)
        spread(c)

    @step("disp0")
    def _():
        pl.loop(SPLIT, SPLIT + EARLY)(spread)
        for c, way in SIDEWAYS:
            fresh(c)
            around(way, c)
        for i, (a, b) in enumerate(pairs):
            pltpu.make_async_copy(a, b, s_w.at[i]).start()
            remote(a, b, s_ws.at[i // 2], s_w.at[i], {"tp": 1 - core}).start()
        pl.loop(SPLIT + EARLY, k)(first)

    @step("preps")
    def _():
        for way in (Z, X, Y):
            landed(met.at[way, pl.ds(1, n - 1)], s_met.at[way])
            for q in range(0 if way != Z else 1, n):
                prep(way, q)

    @step("besxy")
    def _():
        for c, way in SIDEWAYS:
            arrived(c)
            send_tok(way, 2, c, up, 3, 0)
            send_tok(way, 1, c, back, 3, 1)
        for c, way in SIDEWAYS:
            for q in range(3):
                disp(way, q, c)

    @step("besza")
    def _():
        @pl.loop(SPLIT, MIDDLE)
        def _(c):
            arrived(c)
            send_tok(Z, 2, c, up, 3)
            disp(Z, 1, c)
            disp(Z, 2, c)

    @step("acrxy")
    def _():
        for c, way in SIDEWAYS:
            landed(tok.at[3, :, cols(c)], s_tok.at[k + c])
            disp(way, 3, c)

    @step("beszb")
    def _():
        @pl.loop(MIDDLE, k)
        def _(c):
            arrived(c)
            send_tok(Z, 1, c, back, 3)
            disp(Z, 1, c)
            disp(Z, 2, c)

    @step("acrz")
    def _():
        @pl.loop(0, MIDDLE - SPLIT)
        def _(i):
            arrived(k + SPLIT + i)
            disp(Z, 3, SPLIT + i)
            disp(Z, 3, MIDDLE + i)

    @step("weights")
    def _():
        for i, ref in enumerate((wg, wu, wd)):
            landed(ref, s_w.at[i])

    @step("in1")
    def _():
        ready(1)

    @step("gates1")
    def _():
        gates(1)

    @step("down1")
    def _():
        pl.loop(HALF, k)(lambda c: down(1, c))

    @step("in2")
    def _():
        ready(2)

    @step("gates2")
    def _():
        gates(2)

    @step("down2")
    def _():
        pl.loop(0, HALF)(lambda c: down(2, c))

    @step("in3")
    def _():
        ready(3)

    @step("gates3")
    def _():
        gates(3)

    @step("down3")
    def _():
        @pl.loop(0, HALF)
        def _(i):
            down(3, i)
            down(3, i + HALF)
            back_in(2, i)
            combine(1, i + HALF, up, 0, False)
            combine(2, i, back, 1, False)

    @step("down12c3")
    def _():
        @pl.loop(0, HALF)
        def _(i):
            down(1, i)
            down(2, i + HALF)
            back_in(3, i)
            combine(3, i, up, 2, False)
            combine(3, i + HALF, back, 2, False)

    @step("gates0")
    def _():
        ready(0)
        gates(0)

    @step("down0")
    def _():
        pl.loop(0, k)(lambda c: down(0, c))

    @step("comb12b")
    def _():
        @pl.loop(0, HALF)
        def _(i):
            back_in(1, i)
            summed(k + i)
            combine(1, i, up, 0, True)
            combine(2, i + HALF, back, 1, True)

    @step("drain")
    def _():
        landed(met.at[:, pl.ds(1, n - 1)], s_met.at[3])
        landed(wg, s_ws.at[0])
        landed(wd.at[halfrows], s_ws.at[1])
        landed(tok.at[pl.ds(0, n - 1)], s_toks.at[0])
        landed(snd.at[:, pl.ds(0, (side - 1) * cap)], s_xs.at[0])

    @step("last")
    def _():
        @pl.loop(0, k)
        def _(c):
            with jax.named_scope("wr"):
                landed(ret.at[0, pl.ds(0, (side - 1) * cap), cols(c)], s_r.at[pick(0, c)])
            with jax.named_scope("wp"):
                summed(c)
            y = weigh(0, c)
            for slot in (0, 1):
                y = y + racc[slot, c].astype(jnp.float32)
            out[:, cols(c)] = y.astype(out.dtype)

    @step("end")
    def _():
        landed(psend, s_ps.at[0])
        landed(res.at[:, pl.ds(0, (side - 1) * cap)], s_rs.at[0])


def body(
    tokens, norm_gain, norm_bias, gate_weight, up_weight, down_weight, expert_ids, route_weights
):
    count, width = tokens.shape
    experts = lax.axis_size("ep")
    cap = max(4 * count // experts, 4)
    side = experts // LINE
    half = gate_weight.shape[2]
    rows = side * cap
    wide = width // CHUNKS
    bf = jnp.bfloat16
    dma = pltpu.SemaphoreType.DMA
    hbm = pl.BlockSpec(memory_space=pl.ANY)
    return pl.pallas_call(
        functools.partial(kernel, side),
        out_shape=pltpu.VMEM((count, width), bf),
        in_specs=[hbm] * 8,
        out_specs=pl.BlockSpec(memory_space=pltpu.VMEM),
        scratch_shapes=[
            pltpu.VMEM((count, width), bf),
            pltpu.VMEM((1, width), jnp.float32),
            pltpu.VMEM((1, width), jnp.float32),
            pltpu.VMEM((count, 128), jnp.float32),
            pltpu.VMEM((count, 1), jnp.float32),
            pltpu.VMEM((count, 1), jnp.float32),
            pltpu.VMEM((2, count), jnp.int32),
            pltpu.VMEM((2, count), jnp.float32),
            pltpu.VMEM((LINE, count, width), bf),
            pltpu.VMEM((3, LINE, 8, count), jnp.float32),
            pltpu.VMEM((2, width, half), bf),
            pltpu.VMEM((2, width, half), bf),
            pltpu.VMEM((2 * half, width), bf),
            pltpu.VMEM((3, LINE, rows, count), bf),
            pltpu.VMEM((LINE, 2, rows, count), bf),
            pltpu.VMEM((LINE, rows, width), bf),
            pltpu.VMEM((LINE, rows, width), bf),
            pltpu.VMEM((LINE, rows, 2 * half), bf),
            pltpu.VMEM((LINE, rows, width), bf),
            pltpu.VMEM((LINE, rows, width), bf),
            pltpu.VMEM((LINE - 1, CHUNKS, count, wide), bf),
            pltpu.VMEM((LINE - 1, CHUNKS, count, wide), bf),
            dma((5,)),
            dma((4,)),
            dma((3,)),
            dma((2,)),
            dma((CHUNKS + MIDDLE,)),
            dma((1,)),
            dma((2, LINE)),
            dma((1,)),
            dma((2 * CHUNKS + HALF,)),
            dma((1,)),
            dma((CHUNKS + HALF,)),
            dma((1,)),
        ],
        compiler_params=pltpu.CompilerParams(
            collective_id=0, has_side_effects=True, vmem_limit_bytes=52 * 1024 * 1024
        ),
    )(
        *[
            pltpu.with_memory_space_constraint(a, pltpu.HBM)
            for a in (
                tokens, norm_gain[None], norm_bias[None], expert_ids.T, route_weights.T,
                gate_weight, up_weight, down_weight,
            )
        ]
    )


def solution(mesh):
    placed = (
        P(("ep", "tp"), None),
        P(),
        P(),
        P("ep", None, "tp"),
        P("ep", None, "tp"),
        P("ep", "tp", None),
        P(("ep", "tp"), None),
        P(("ep", "tp"), None),
    )
    return jax.shard_map(
        body, mesh=mesh, in_specs=placed, out_specs=P(("ep", "tp"), None), check_vma=False
    )
```

```python
import functools

import jax
import jax.numpy as jnp
from jax import lax
from jax.experimental import pallas as pl
from jax.experimental.pallas import tpu as pltpu
from jax.sharding import PartitionSpec as P

MESH = pl.DeviceIdType.MESH
LINE = 4
CHUNKS = 8
HALF = CHUNKS // 2
EARLY = 1
X, Y, Z = 0, 1, 2
SIDEWAYS = [(0, X), (1, Y)]
SPLIT = len(SIDEWAYS)
MIDDLE = (SPLIT + CHUNKS) // 2


def kernel(
    planes, raw, gain, bias, idsin, wtin, gw, uw, dw, out,
    src, gn, bs, part, mu, rs, ids, wts, tok, met, wg, wu, wd, sel, mix, snd, xin, hid, res, ret, psend, racc,
    s_own, s_met, s_w, s_ws, s_tok, s_toks, s_x, s_xs, s_r, s_rs, s_p, s_ps,
):
    n = LINE
    side = planes
    me, core = lax.axis_index("ep"), lax.axis_index("tp")
    z, p = me // side, lax.rem(me, side)
    y, x = p // LINE, lax.rem(p, LINE)
    tokens, width = raw.shape
    half = gw.shape[2]
    rows = snd.shape[1]
    cap = rows // side
    k = CHUNKS
    wide = width // k

    def cols(c):
        return pl.ds(pl.multiple_of(c * wide, wide), wide)

    def band(i):
        return pl.ds(pl.multiple_of(i * cap, cap), cap)

    def plane(j):
        return {"ep": lax.rem(z + j, n) * side + p}

    up, over, back = 1, 2, n - 1
    role = {0: 0, up: 1, back: 2, over: 3}
    steps = {q: j for j, q in role.items()}

    def ident(a, b, c):
        return {"ep": a * side + b * n + c}

    def turn(a, j):
        return lax.rem(a + j, n) if j else a

    def ring(way, j):
        return ident(
            turn(z, j if way == Z else 0), turn(y, j if way == Y else 0), turn(x, j if way == X else 0)
        )


    def away(d):
        return sum(min(j, n - j) for j in d)

    offsets = [(b, c) for b in range(n) for c in range(n) if b or c]
    peers = [
        lax.rem(y + b, n) * n + lax.rem(x + c, n)
        for b, c in sorted(offsets, key=lambda d: -away(d))
    ]

    def remote(src, dst, send, recv, where):
        return pltpu.make_async_remote_copy(
            src_ref=src, dst_ref=dst, send_sem=send, recv_sem=recv,
            device_id=where, device_id_type=MESH,
        )

    def landed(ref, sem):
        pltpu.make_async_copy(ref, ref, sem).wait()

    def step(name):
        def run(f):
            with jax.named_scope(name):
                f()
        return run

    firsts = [
        pltpu.make_async_copy(a, b, s_own.at[i])
        for i, (a, b) in enumerate(
            [(raw, src), (gain, gn), (bias, bs), (idsin, ids), (wtin, wts)]
        )
    ]
    for copy in firsts:
        copy.start()
    barrier = pltpu.get_barrier_semaphore()
    for o in peers:
        pl.semaphore_signal(barrier, inc=1, device_id={"ep": z * side + o}, device_id_type=MESH)
    for j in range(1, n):
        pl.semaphore_signal(barrier, inc=1, device_id=plane(j), device_id_type=MESH)
    pl.semaphore_signal(barrier, inc=1, device_id={"tp": 1 - core}, device_id_type=MESH)

    def send_tok(way, q, c, to, slot, part=None):
        if slot < 3:
            count = c
        elif way == Z:
            count = k + SPLIT + lax.rem(c - SPLIT, MIDDLE - SPLIT)
        else:
            count = k + c
        at = cols(c)
        if part is not None:
            at = pl.ds(c * wide + part * (wide // 2), wide // 2)
        remote(
            tok.at[q, :, at], tok.at[slot, :, at], s_toks.at[0], s_tok.at[count], ring(way, to)
        ).start()

    def prep(way, q):
        at = (way, q) if q else (Z, 0)
        ids0, ids1 = met[at + (slice(0, 1),)], met[at + (slice(1, 2),)]
        wt0, wt1 = met[at + (slice(2, 3),)], met[at + (slice(3, 4),)]
        row = lax.broadcasted_iota(jnp.int32, (rows, tokens), 0)
        which = row // cap
        far, close = which // n, lax.rem(which, n)
        expert = [
            far * side + close * n + x, far * side + y * n + close, z * side + which
        ][way]
        e_row = expert.astype(jnp.float32)
        s_row = lax.rem(row, cap).astype(jnp.float32)
        hit0 = (ids0 == e_row).astype(jnp.float32)
        hit1 = (ids1 == e_row).astype(jnp.float32)
        hit = hit0 + hit1
        before = (
            lax.broadcasted_iota(jnp.int32, (tokens, tokens), 0)
            < lax.broadcasted_iota(jnp.int32, (tokens, tokens), 1)
        ).astype(jnp.float32).astype(jnp.bfloat16)
        count = jnp.dot(hit.astype(jnp.bfloat16), before, preferred_element_type=jnp.float32)
        pick = jnp.where(count == s_row, hit, 0.0)
        sel[way, q] = pick.astype(jnp.bfloat16)
        if way == Z:
            w = pick * (hit0 * wt0 + hit1 * wt1)
            high = w.astype(jnp.bfloat16)
            mix[q, 0] = high
            mix[q, 1] = (w - high.astype(jnp.float32)).astype(jnp.bfloat16)

    @step("prep0")
    def _():
        for copy in firsts[3:]:
            copy.wait()
        met[Z, 0, 0:2, :] = ids[...].astype(jnp.float32)
        met[Z, 0, 2:4, :] = wts[...]
        met[Z, 0, 4:8, :] = jnp.zeros((4, tokens), jnp.float32)
        prep(Z, 0)

    @step("raw")
    def _():
        for copy in firsts[:3]:
            copy.wait()

    slab = min(16, tokens)
    lanes = part.shape[1]

    @step("stats")
    def _():
        def total(i, f):
            at = pl.ds(pl.multiple_of(i * slab, slab), slab)
            parts = [
                f(src[at, j * lanes : (j + 1) * lanes].astype(jnp.float32), at)
                for j in range(width // lanes)
            ]
            while len(parts) > 1:
                parts = [a + b for a, b in zip(parts[::2], parts[1::2])]
            part[at, :] = parts[0]

        pl.loop(0, tokens // slab)(lambda i: total(i, lambda v, at: v))
        mu[...] = jnp.sum(part[...], axis=-1, keepdims=True) / width

        def square(v, at):
            v = v - mu[at, :]
            return v * v

        pl.loop(0, tokens // slab)(lambda i: total(i, square))
        rs[...] = lax.rsqrt(jnp.sum(part[...], axis=-1, keepdims=True) / width + 1e-05)

    def fresh(c):
        v = (src[:, cols(c)].astype(jnp.float32) - mu[...]) * rs[...]
        tok[0, :, cols(c)] = (v * gn[:, cols(c)] + bs[:, cols(c)]).astype(jnp.bfloat16)

    def select(way, q, c):
        v = jnp.dot(sel[way, q], tok[q, :, cols(c)], preferred_element_type=jnp.float32)
        snd[q, :, cols(c)] = v.astype(jnp.bfloat16)

    def ship(way, q, c):
        if way == Z:
            xin[q, band(p), cols(c)] = snd[q, band(p), cols(c)]
            for o in peers:
                remote(
                    snd.at[q, band(o), cols(c)], xin.at[q, band(p), cols(c)],
                    s_xs.at[0], s_x.at[1, q], {"ep": z * side + o},
                ).start()
            return
        j = steps[q]
        for a, b in [(0, 0)] + sorted(offsets, key=lambda d: -away(d)):
            far = turn(z, a)
            if way == X:
                close = turn(y, b)
                where, to = ident(far, close, x), y * n + turn(x, j)
            else:
                close = turn(x, b)
                where, to = ident(far, y, close), turn(y, j) * n + x
            got = xin.at[role[(n - a) % n], band(to), cols(c)]
            row = band(far * n + close)
            if a or b:
                remote(
                    snd.at[q, row, cols(c)], got, s_xs.at[0], s_x.at[0, role[(n - a) % n]], where
                ).start()
            else:
                xin[0, band(to), cols(c)] = snd[q, row, cols(c)]

    def disp(way, q, c):
        select(way, q, c)
        ship(way, q, c)

    def ready(q):
        count = (side - n if q == 0 else side) * cap
        landed(xin.at[q, pl.ds(0, count), pl.ds(0, SPLIT * wide)], s_x.at[0, q])
        landed(xin.at[q, pl.ds(0, (side - 1) * cap), pl.ds(SPLIT * wide, (k - SPLIT) * wide)], s_x.at[1, q])

    @step("early")
    def _():
        for c in range(SPLIT, SPLIT + EARLY):
            fresh(c)
            select(Z, 0, c)

    @step("meet")
    def _():
        pl.semaphore_wait(barrier, side - 1 + n)

    @step("own")
    def _():
        for way in (Z, X, Y):
            for q in range(1, n):
                slot = role[n - steps[q]]
                remote(
                    met.at[Z, 0], met.at[way, slot], s_met.at[3], s_met.at[way], ring(way, steps[q])
                ).start()

    def others(ref, q):
        return ref.at[q, pl.ds(0, (side - 1) * cap)]

    tile = min(256, half)
    per = half // tile

    def gate(q, i):
        h, at = i // per, lax.rem(i, per)
        part = pl.ds(pl.multiple_of(at * tile, tile), tile)
        x = xin[q]
        g = jnp.dot(x, wg[h, :, part], preferred_element_type=jnp.float32)
        u = jnp.dot(x, wu[h, :, part], preferred_element_type=jnp.float32)
        v = g / (1.0 + jnp.exp(-g)) * u
        hid[q, :, pl.ds(pl.multiple_of(i * tile, tile), tile)] = v.astype(jnp.bfloat16)

    def gates(q):
        pl.loop(0, 2 * per)(lambda i: gate(q, i))

    def product(q, c):
        y = jnp.dot(hid[q], wd[:, cols(c)], preferred_element_type=jnp.float32)
        res[q, :, cols(c)] = y.astype(jnp.bfloat16)
        ret[q, band(p), cols(c)] = res[q, band(p), cols(c)]

    def pick(q, c):
        if q == 0:
            return c
        if q == 3:
            return k + lax.rem(c, HALF)
        return k + HALF + lax.rem(c + (HALF if q == 1 else 0), k)

    def give(q, c):
        for o in peers:
            remote(
                res.at[q, band(o), cols(c)], ret.at[q, band(p), cols(c)],
                s_rs.at[0], s_r.at[pick(q, c)], {"ep": z * side + o},
            ).start()

    def down(q, c):
        product(q, c)
        give(q, c)

    def weigh(q, c):
        r = ret[q, :, cols(c)]
        dims = (((0,), (0,)), ((), ()))
        return lax.dot_general(
            mix[q, 0], r, dims, preferred_element_type=jnp.float32
        ) + lax.dot_general(mix[q, 1], r, dims, preferred_element_type=jnp.float32)

    def combine(q, c, to, slot, add):
        v = weigh(q, c)
        if add:
            v = v + racc[2, c].astype(jnp.float32)
        psend[q - 1, c] = v.astype(jnp.bfloat16)
        count = k + lax.rem(c, HALF) if slot == 2 else c
        remote(
            psend.at[q - 1, c], racc.at[slot, c], s_ps.at[0], s_p.at[count], plane(to)
        ).start()

    def back_in(q, c):
        landed(ret.at[q, pl.ds(0, (side - 1) * cap), pl.ds(0, 2 * wide)], s_r.at[pick(q, c)])

    def summed(i):
        landed(racc.at[0, pl.ds(0, 2)], s_p.at[i])

    def arrived(i):
        landed(tok.at[1, :, pl.ds(0, 2 * wide)], s_tok.at[i])

    halfrows = pl.ds(pl.multiple_of(core * half, half), half)
    pairs = [
        (gw.at[0], wg.at[core]), (uw.at[0], wu.at[core]), (dw.at[0], wd.at[halfrows]),
    ]

    def around(way, c):
        send_tok(way, 0, c, up, 2)
        send_tok(way, 0, c, back, 1)

    def spread(c):
        around(Z, c)
        ship(Z, 0, c)

    def first(c):
        fresh(c)
        select(Z, 0, c)
        spread(c)

    @step("disp0")
    def _():
        pl.loop(SPLIT, SPLIT + EARLY)(spread)
        for c, way in SIDEWAYS:
            fresh(c)
            around(way, c)
        for i, (a, b) in enumerate(pairs):
            pltpu.make_async_copy(a, b, s_w.at[i]).start()
            remote(a, b, s_ws.at[i // 2], s_w.at[i], {"tp": 1 - core}).start()
        pl.loop(SPLIT + EARLY, k)(first)

    @step("preps")
    def _():
        for way in (Z, X, Y):
            landed(met.at[way, pl.ds(1, n - 1)], s_met.at[way])
            for q in range(0 if way != Z else 1, n):
                prep(way, q)

    @step("besxy")
    def _():
        for c, way in SIDEWAYS:
            arrived(c)
            send_tok(way, 2, c, up, 3, 0)
            send_tok(way, 1, c, back, 3, 1)
        for c, way in SIDEWAYS:
            for q in range(3):
                disp(way, q, c)

    @step("besza")
    def _():
        @pl.loop(SPLIT, MIDDLE)
        def _(c):
            arrived(c)
            send_tok(Z, 2, c, up, 3)
            disp(Z, 1, c)
            disp(Z, 2, c)

    @step("acrxy")
    def _():
        for c, way in SIDEWAYS:
            landed(tok.at[3, :, cols(c)], s_tok.at[k + c])
            disp(way, 3, c)

    @step("beszb")
    def _():
        @pl.loop(MIDDLE, k)
        def _(c):
            arrived(c)
            send_tok(Z, 1, c, back, 3)
            disp(Z, 1, c)
            disp(Z, 2, c)

    @step("acrz")
    def _():
        @pl.loop(0, MIDDLE - SPLIT)
        def _(i):
            arrived(k + SPLIT + i)
            disp(Z, 3, SPLIT + i)
            disp(Z, 3, MIDDLE + i)

    @step("weights")
    def _():
        for i, ref in enumerate((wg, wu, wd)):
            landed(ref, s_w.at[i])

    @step("in1")
    def _():
        ready(1)

    @step("gates1")
    def _():
        gates(1)

    @step("down1")
    def _():
        pl.loop(HALF, k)(lambda c: down(1, c))

    @step("in2")
    def _():
        ready(2)

    @step("gates2")
    def _():
        gates(2)

    @step("down2")
    def _():
        pl.loop(0, HALF)(lambda c: down(2, c))

    @step("in3")
    def _():
        ready(3)

    @step("gates3")
    def _():
        gates(3)

    @step("down3")
    def _():
        @pl.loop(0, HALF)
        def _(i):
            down(3, i)
            down(3, i + HALF)
            back_in(2, i)
            combine(1, i + HALF, up, 0, False)
            combine(2, i, back, 1, False)

    @step("down12c3")
    def _():
        @pl.loop(0, HALF)
        def _(i):
            down(1, i)
            down(2, i + HALF)
            back_in(3, i)
            combine(3, i, up, 2, False)
            combine(3, i + HALF, back, 2, False)

    @step("gates0")
    def _():
        ready(0)
        gates(0)

    @step("down0")
    def _():
        pl.loop(0, k)(lambda c: down(0, c))

    @step("comb12b")
    def _():
        @pl.loop(0, HALF)
        def _(i):
            back_in(1, i)
            summed(k + i)
            combine(1, i, up, 0, True)
            combine(2, i + HALF, back, 1, True)

    @step("drain")
    def _():
        landed(met.at[:, pl.ds(1, n - 1)], s_met.at[3])
        landed(wg, s_ws.at[0])
        landed(wd.at[halfrows], s_ws.at[1])
        landed(tok.at[pl.ds(0, n - 1)], s_toks.at[0])
        landed(snd.at[:, pl.ds(0, (side - 1) * cap)], s_xs.at[0])

    @step("last")
    def _():
        @pl.loop(0, k)
        def _(c):
            with jax.named_scope("wr"):
                landed(ret.at[0, pl.ds(0, (side - 1) * cap), cols(c)], s_r.at[pick(0, c)])
            with jax.named_scope("wp"):
                summed(c)
            y = weigh(0, c)
            for slot in (0, 1):
                y = y + racc[slot, c].astype(jnp.float32)
            out[:, cols(c)] = y.astype(out.dtype)

    @step("end")
    def _():
        landed(psend, s_ps.at[0])
        landed(res.at[:, pl.ds(0, (side - 1) * cap)], s_rs.at[0])


def body(
    tokens, norm_gain, norm_bias, gate_weight, up_weight, down_weight, expert_ids, route_weights
):
    count, width = tokens.shape
    experts = lax.axis_size("ep")
    cap = max(4 * count // experts, 4)
    side = experts // LINE
    half = gate_weight.shape[2]
    rows = side * cap
    wide = width // CHUNKS
    bf = jnp.bfloat16
    dma = pltpu.SemaphoreType.DMA
    hbm = pl.BlockSpec(memory_space=pl.ANY)
    return pl.pallas_call(
        functools.partial(kernel, side),
        out_shape=pltpu.VMEM((count, width), bf),
        in_specs=[hbm] * 8,
        out_specs=pl.BlockSpec(memory_space=pltpu.VMEM),
        scratch_shapes=[
            pltpu.VMEM((count, width), bf),
            pltpu.VMEM((1, width), jnp.float32),
            pltpu.VMEM((1, width), jnp.float32),
            pltpu.VMEM((count, 128), jnp.float32),
            pltpu.VMEM((count, 1), jnp.float32),
            pltpu.VMEM((count, 1), jnp.float32),
            pltpu.VMEM((2, count), jnp.int32),
            pltpu.VMEM((2, count), jnp.float32),
            pltpu.VMEM((LINE, count, width), bf),
            pltpu.VMEM((3, LINE, 8, count), jnp.float32),
            pltpu.VMEM((2, width, half), bf),
            pltpu.VMEM((2, width, half), bf),
            pltpu.VMEM((2 * half, width), bf),
            pltpu.VMEM((3, LINE, rows, count), bf),
            pltpu.VMEM((LINE, 2, rows, count), bf),
            pltpu.VMEM((LINE, rows, width), bf),
            pltpu.VMEM((LINE, rows, width), bf),
            pltpu.VMEM((LINE, rows, 2 * half), bf),
            pltpu.VMEM((LINE, rows, width), bf),
            pltpu.VMEM((LINE, rows, width), bf),
            pltpu.VMEM((LINE - 1, CHUNKS, count, wide), bf),
            pltpu.VMEM((LINE - 1, CHUNKS, count, wide), bf),
            dma((5,)),
            dma((4,)),
            dma((3,)),
            dma((2,)),
            dma((CHUNKS + MIDDLE,)),
            dma((1,)),
            dma((2, LINE)),
            dma((1,)),
            dma((2 * CHUNKS + HALF,)),
            dma((1,)),
            dma((CHUNKS + HALF,)),
            dma((1,)),
        ],
        compiler_params=pltpu.CompilerParams(
            collective_id=0, has_side_effects=True, vmem_limit_bytes=52 * 1024 * 1024
        ),
    )(
        *[
            pltpu.with_memory_space_constraint(a, pltpu.HBM)
            for a in (
                tokens, norm_gain[None], norm_bias[None], expert_ids.T, route_weights.T,
                gate_weight, up_weight, down_weight,
            )
        ]
    )


def solution(mesh):
    placed = (
        P(("ep", "tp"), None),
        P(),
        P(),
        P("ep", None, "tp"),
        P("ep", None, "tp"),
        P("ep", "tp", None),
        P(("ep", "tp"), None),
        P(("ep", "tp"), None),
    )
    return jax.shard_map(
        body, mesh=mesh, in_specs=placed, out_specs=P(("ep", "tp"), None), check_vma=False
    )
```
